32 devices in a mesh: sp: 8 (over z, core), tp: 4 (over y, x).
Axes of the slice: x: 2, y: 2, z: 4, core: 2. Of those that a mesh axis runs over, the one named last changes fastest.
Arguments:
- query_pairs: bfloat16 [2048, 2048], P('sp', 'tp'), may hold values from -8 to 8
- key_pairs: bfloat16 [2048, 2048], P('sp', 'tp'), may hold values from -6 to 6
- value_rows: bfloat16 [2048, 2048], P('sp', 'tp'), may hold values from -6 to 6
- doc_ids: int32 [2048], P('sp'), may hold values from 0 to 3, never falling along the last dimension, each value on 1 to 1280 neighbouring positions
- contrast_lambda: float32 [32], P('tp'), may hold values from 0.3 to 0.8
- head_gain: float32 [64], replicated, may hold values from 0.1 to 1.9
- stream: bfloat16 [2048, 2048], P('sp', 'tp'), may hold values from -6 to 6
- out_proj: bfloat16 [2048, 2048], P(None, 'tp'), may hold values from -0.125 to 0.125
- norm_gain: float32 [2048], replicated, may hold values from 0.1 to 1.9
- routes: int32 [2048, 2], P('sp'), may hold values from 0 to 7, all different within a row; in each aligned block of 256 rows (0 to 255, 256 to 511, ...) at most 128 rows name the same one
- route_weights: float32 [2048, 2], P('sp'), may hold values from 0.3 to 1.5
- expert_gate: bfloat16 [8, 2048, 2048], P('sp', None, 'tp'), may hold values from -0.125 to 0.125
- expert_up: bfloat16 [8, 2048, 2048], P('sp', None, 'tp'), may hold values from -0.125 to 0.125
- expert_down: bfloat16 [8, 2048, 2048], P('sp', None, 'tp'), may hold values from -0.125 to 0.125
- shared_gate: bfloat16 [2048, 2048], P(None, 'tp'), may hold values from -0.125 to 0.125
- shared_up: bfloat16 [2048, 2048], P(None, 'tp'), may hold values from -0.125 to 0.125
- shared_down: bfloat16 [2048, 2048], P(None, 'tp'), may hold values from -0.125 to 0.125
Outputs:
- mixed: bfloat16 [2048, 2048], P('sp', 'tp')
The draws below stay inside these ranges and needn't reach their ends.
Inputs may be any that keep to these rules, and one draw needn't show every extreme that they name: `doc_ids`: document numbers never fall along the positions; a document holds at most 1280 positions. `routes`: A position names 2 different experts. In each aligned block of 256 rows no expert is named by more than 128 rows, and every draw has a block in which some expert is named by exactly 128 rows.
All inputs are finite; a program needn't handle non-finite values.
Results may differ from the reference program's by a relative error of at most 0.011.
Values may be sent and summed in bfloat16 or wider, within the bound.
No kernel may reach another device: no remote copies, remote signals or barrier semaphores. Data moves between devices by JAX's collectives and lax.ppermute only.
A program may use at most 64 MiB of HBM per device.

```python
import math
import jax
import jax.numpy as jnp
import numpy as np
from jax import lax

D = 2048
HEADS = 32
QK = 32
V = 64
FE = 2048
FS = 2048
TOP_K = 2
TOK_DEV = 256
TOKENS = 2048
EXPERTS = 8
CAP = 128
DOC_COUNT = 4
DOC_MOST = 1280
N_SP = 8


def paired_fields(key):
    base = jax.random.fold_in(key, 4321)
    query_seed, key_seed = jax.random.split(base, 2)
    shape = (TOKENS, HEADS, 2, QK)
    queries = jnp.clip(1.3 * jax.random.normal(query_seed, shape, jnp.float32), -6.0, 6.0)
    keys = jnp.clip(1.3 * jax.random.normal(key_seed, shape, jnp.float32), -6.0, 6.0)
    return (queries.reshape(TOKENS, HEADS * 2 * QK), keys.reshape(TOKENS, HEADS * 2 * QK))


def draw_query_pairs(key, part):
    return paired_fields(key)[0].astype(jnp.bfloat16)


def draw_key_pairs(key, part):
    return paired_fields(key)[1].astype(jnp.bfloat16)


def steps_of(rng, dims, cuts, low, high):
    loudness, own = 1.0, jax.random.fold_in(rng, 6)
    for axis_at, shards_of in cuts:
        draws = jnp.exp(jax.random.uniform(jax.random.fold_in(own, axis_at), (shards_of,), jnp.float32, low / len(cuts), high / len(cuts)))
        loudness = loudness * jnp.repeat(draws, dims[axis_at] // shards_of).reshape([-1 if axis == axis_at else 1 for axis in range(len(dims))])
    return loudness


def profile(count, total, most, lean):
    loads = [(1 << 20) // math.isqrt(rank ** lean) + 1 for rank in range(2, count + 1)]
    spare, holding = total - most - (count - 1), [1] * (count - 1)
    while spare > 0:
        free = [i for i in range(count - 1) if holding[i] < most]
        mass, remaining = sum([loads[i] for i in free]), spare
        for i in free:
            addition = min(most - holding[i], max(1, remaining * loads[i] // mass), spare)
            holding[i] = holding[i] + addition
            spare = spare - addition
    return np.array([most] + holding)


def uneven_parts(key, count, total, bound, skew):
    if count == 2:
        one = jax.random.randint(key, (), max(1, total - bound), min(bound, total - 1) + 1)
        return jnp.stack([one, total - one])
    sizes = jnp.asarray(profile(count, total, bound, skew), jnp.int32)
    pairs = (count - 1) // 2
    donor, receiver = sizes[1:1 + 2 * pairs:2], sizes[2:2 + 2 * pairs:2]
    slack = jnp.minimum(donor - 1, bound - receiver)
    shifted = jax.random.randint(jax.random.fold_in(key, 1), (pairs,), 0, 1 << 20) % (slack + 1)
    sizes = sizes.at[1:1 + 2 * pairs:2].set(donor - shifted).at[2:2 + 2 * pairs:2].set(receiver + shifted)
    return sizes[jax.random.permutation(jax.random.fold_in(key, 2), count)]


def assign_block(own_key, own, number, rows, number_of, top, most, lean):
    order = jax.random.permutation(own_key, number_of)
    crowded, ordinary = shares(number_of, rows * top, most, lean, True), shares(number_of, rows * top, most, lean, False)
    places = jnp.arange(number_of)

    def named(lengths, turn):
        used = int((lengths > 0).sum())
        fixed = max(1, used // 4)
        moved = fixed + (places - fixed + turn * (used - fixed)) % max(1, number_of - fixed)
        return jnp.zeros((number_of,), jnp.int32).at[order[jnp.where(places < fixed, places, moved)]].set(jnp.asarray(lengths, jnp.int32))

    lengths = jnp.where(number % 4 == 0, named(crowded, number // 4), named(ordinary, number - number // 4 - 1))
    mixed = jax.random.permutation(jax.random.fold_in(own, 3), number_of)
    donor, taker = mixed[0:number_of // 2 * 2:2], mixed[1:number_of // 2 * 2:2]
    margin = jnp.minimum(lengths[donor] - 1, most - lengths[taker]) // 2
    margin = jnp.where((donor == order[0]) | (taker == order[0]) | (lengths[taker] == 0), 0, jnp.maximum(margin, 0))
    moved = jax.random.randint(jax.random.fold_in(own, 4), (number_of // 2,), 0, 1 << 20) % (margin + 1)
    lengths = lengths.at[donor].add(-moved).at[taker].add(moved)
    members = jnp.searchsorted(jnp.cumsum(lengths), jnp.arange(rows * top), side="right").astype(jnp.int32)
    grid = members.reshape(top, rows).T
    grid = grid[jax.random.permutation(jax.random.fold_in(own, 1), rows)]
    turn = jax.random.randint(jax.random.fold_in(own, 2), (rows, 1), 0, top)
    return jnp.take_along_axis(grid, (jnp.arange(top)[None, :] + turn) % top, axis=1)


def shares(count, total, reach, lean, full):
    loads = [(1 << 20) // math.isqrt(grade ** lean) + 1 for grade in range(1, count + 1)]
    largest = reach if full else min(reach, max(-(-total // count), total * loads[0] // sum(loads)))
    least = 1 if total - largest >= count - 1 else 0
    given, spare = [largest] + [least] * (count - 1), total - largest - least * (count - 1)
    while spare > 0:
        candidates = [i for i in range(1, count) if given[i] < largest] or [i for i in range(1, count) if given[i] < reach]
        mass, left = sum([loads[i] for i in candidates]), spare
        for i in candidates:
            extra = min(reach - given[i], max(1, left * loads[i] // mass), spare)
            given[i] = given[i] + extra
            spare = spare - extra
    return np.array(given)


def bell_draw(rng, dims, deviation, reach, pieces=(), kind=jnp.bfloat16):
    entries = deviation * jax.random.normal(rng, dims, jnp.float32)
    if pieces:
        entries = entries * steps_of(rng, dims, pieces, -0.22, 0.18)
    return jnp.clip(entries, -reach, reach).astype(kind)


def setup_inputs(seed: int = 0) -> dict:
    splits = jax.random.split(jax.random.key(seed), 18)
    query_pairs = draw_query_pairs(jax.random.fold_in(splits[17], 71), 0)
    key_pairs = draw_key_pairs(jax.random.fold_in(splits[17], 71), 0)
    value_rows = bell_draw(splits[2], (TOKENS, HEADS * V), 1.0, 6.0, ((0, 8), (1, 4)))
    doc_ids = jnp.searchsorted(jnp.cumsum(uneven_parts(splits[3], DOC_COUNT, TOKENS, DOC_MOST, 1)), jnp.arange(TOKENS), side="right").astype(jnp.int32)
    contrast_lambda = jnp.clip(0.3 + 0.5 * jax.random.uniform(splits[4], (HEADS,), jnp.float32) ** steps_of(splits[4], (HEADS,), ((0, 4),), -0.2, 0.2), 0.3, 0.8)
    head_gain = jnp.clip(1.0 + 0.18 * jax.random.normal(splits[5], (V,), jnp.float32), 0.1, 1.9)
    stream = bell_draw(splits[6], (TOKENS, D), 1.0, 6.0, ((0, 8), (1, 4)))
    out_proj = bell_draw(splits[7], (HEADS * V, D), (HEADS * V) ** -0.5, 0.125, ((1, 4),))
    norm_gain = jnp.clip(1.0 + 0.18 * jax.random.normal(splits[8], (D,), jnp.float32), 0.1, 1.9)
    routes_keys = jax.random.split(jax.random.fold_in(splits[9], 1), TOKENS // TOK_DEV)
    routes_turns = jax.random.permutation(jax.random.fold_in(splits[9], 3), TOKENS // TOK_DEV)
    routes = jax.vmap(lambda own, number: assign_block(jax.random.fold_in(splits[9], 2), own, number, TOK_DEV, EXPERTS, TOP_K, CAP, 2))(routes_keys, routes_turns).reshape((TOKENS, TOP_K))
    route_weights = jnp.clip(0.3 + 1.2 * jax.random.uniform(splits[10], (TOKENS, TOP_K), jnp.float32) ** steps_of(splits[10], (TOKENS, TOP_K), ((0, 8),), -0.2, 0.2), 0.3, 1.5)
    expert_gate = bell_draw(splits[11], (EXPERTS, D, FE), D ** -0.5, 0.125, ((0, 8), (2, 4)))
    expert_up = bell_draw(splits[12], (EXPERTS, D, FE), D ** -0.5, 0.125, ((0, 8), (2, 4)))
    expert_down = bell_draw(splits[13], (EXPERTS, FE, D), FE ** -0.5, 0.125, ((0, 8), (2, 4)))
    shared_gate = bell_draw(splits[14], (D, FS), D ** -0.5, 0.125, ((1, 4),))
    shared_up = bell_draw(splits[15], (D, FS), D ** -0.5, 0.125, ((1, 4),))
    shared_down = bell_draw(splits[16], (FS, D), FS ** -0.5, 0.125, ((1, 4),))
    return {"query_pairs": query_pairs, "key_pairs": key_pairs, "value_rows": value_rows, "doc_ids": doc_ids, "contrast_lambda": contrast_lambda, "head_gain": head_gain, "stream": stream, "out_proj": out_proj, "norm_gain": norm_gain, "routes": routes, "route_weights": route_weights, "expert_gate": expert_gate, "expert_up": expert_up, "expert_down": expert_down, "shared_gate": shared_gate, "shared_up": shared_up, "shared_down": shared_down}


epsilon = 1e-06
floor_score = -1e+30

def attend(query_pairs, key_pairs, value_rows, doc_ids, contrast_lambda, head_gain):
    query_heads = jnp.transpose(query_pairs.reshape(TOKENS, HEADS, 2, QK), (1, 0, 2, 3)).astype(jnp.float32)
    key_heads = jnp.transpose(key_pairs.reshape(TOKENS, HEADS, 2, QK), (1, 0, 2, 3)).astype(jnp.float32)
    value_heads = jnp.transpose(value_rows.reshape(TOKENS, HEADS, V), (1, 0, 2)).astype(jnp.float32)
    positions = jnp.arange(TOKENS, dtype=jnp.int32)
    block_starts = jnp.arange(TOKENS // TOK_DEV, dtype=jnp.int32) * TOK_DEV

    def one_head(operands):
        queries, keys, values, weight = operands

        def one_block(block_start):
            block_query = lax.dynamic_slice_in_dim(queries, block_start, TOK_DEV, 0)
            block_pos = lax.dynamic_slice_in_dim(positions, block_start, TOK_DEV, 0)
            block_doc = lax.dynamic_slice_in_dim(doc_ids, block_start, TOK_DEV, 0)
            allowed = (positions[None, :] <= block_pos[:, None]) & (doc_ids[None, :] == block_doc[:, None])
            scores = jnp.einsum('qmd,kmd->mqk', block_query, keys) * QK ** (-0.5)
            scores = jnp.where(allowed, scores, floor_score)
            row_peak = lax.optimization_barrier(jnp.max(scores, axis=-1, keepdims=True))
            weights = jnp.where(allowed, jnp.exp(scores - row_peak), 0.0)
            rounded = lax.optimization_barrier(weights.astype(jnp.bfloat16)).astype(jnp.float32)
            heard = jnp.einsum('mqk,kv->mqv', rounded, values) / lax.optimization_barrier(jnp.sum(weights, axis=-1))[..., None]
            contrast = heard[0] - weight * heard[1]
            contrast = contrast * lax.rsqrt(lax.optimization_barrier(jnp.mean(contrast * contrast, axis=-1, keepdims=True)) + epsilon) * head_gain
            return contrast.astype(jnp.bfloat16)
        return lax.map(one_block, block_starts).reshape(TOKENS, V)
    heads = lax.map(one_head, (query_heads, key_heads, value_heads, contrast_lambda))
    return jnp.transpose(heads, (1, 0, 2)).reshape(TOKENS, HEADS * V)

def reference(query_pairs, key_pairs, value_rows, doc_ids, contrast_lambda, head_gain, stream, out_proj, norm_gain, routes, route_weights, expert_gate, expert_up, expert_down, shared_gate, shared_up, shared_down):
    head_out = attend(query_pairs, key_pairs, value_rows, doc_ids, contrast_lambda, head_gain)
    hidden_state = (stream.astype(jnp.float32) + jnp.dot(head_out, out_proj, preferred_element_type=jnp.float32)).astype(jnp.bfloat16)
    widened = hidden_state.astype(jnp.float32)
    normed = (widened * lax.rsqrt(lax.optimization_barrier(jnp.mean(widened * widened, axis=-1, keepdims=True)) + epsilon) * norm_gain).astype(jnp.bfloat16)
    shared_act = (jax.nn.silu(jnp.dot(normed, shared_gate, preferred_element_type=jnp.float32)) * jnp.dot(normed, shared_up, preferred_element_type=jnp.float32)).astype(jnp.bfloat16)
    shared_part = jnp.dot(shared_act, shared_down, preferred_element_type=jnp.float32)
    most_rows = N_SP * CAP

    def one_expert(running, operands):
        gate_weight, up_weight, down_weight, expert = operands
        matches = routes == expert
        picked = jnp.any(matches, axis=1)
        portion = lax.optimization_barrier(jnp.sum(jnp.where(matches, route_weights, 0.0), axis=1))
        chosen = jnp.nonzero(picked, size=most_rows, fill_value=0)[0].astype(jnp.int32)
        live = (jnp.arange(most_rows, dtype=jnp.int32) < jnp.sum(picked.astype(jnp.int32))).astype(jnp.float32)
        inputs = normed[chosen]
        expert_act = (jax.nn.silu(jnp.dot(inputs, gate_weight, preferred_element_type=jnp.float32)) * jnp.dot(inputs, up_weight, preferred_element_type=jnp.float32)).astype(jnp.bfloat16)
        expert_out = jnp.dot(expert_act, down_weight, preferred_element_type=jnp.float32).astype(jnp.bfloat16)
        scaled = expert_out.astype(jnp.float32) * (portion[chosen] * live)[:, None]
        return (running.at[chosen].add(scaled), None)
    routed, _ = lax.scan(one_expert, jnp.zeros((TOKENS, D), jnp.float32), (expert_gate, expert_up, expert_down, jnp.arange(EXPERTS, dtype=jnp.int32)))
    return (widened + shared_part + routed).astype(jnp.bfloat16)
```

```python
import functools

import jax
import jax.numpy as jnp
from jax import lax
from jax.experimental import pallas as pl
from jax.experimental.pallas import tpu as pltpu
from jax.sharding import PartitionSpec as P

epsilon = 1e-06
floor_score = -1e30


def add_columns(weight_rows, part_block):
    return jnp.dot(part_block, weight_rows, preferred_element_type=jnp.float32)


def shards(
    query_pairs,
    key_pairs,
    value_rows,
    doc_ids,
    contrast_lambda,
    head_gain,
    stream,
    out_proj,
    norm_gain,
    routes,
    route_weights,
    expert_gate,
    expert_up,
    expert_down,
    shared_gate,
    shared_up,
    shared_down,
):
    row_count = query_pairs.shape[0]
    local_heads = contrast_lambda.shape[0]
    key_width = query_pairs.shape[1] // (2 * local_heads)
    value_width = value_rows.shape[1] // local_heads
    scaling = key_width ** (-0.5)
    first_row = lax.axis_index("sp") * row_count
    query_pos = first_row + jnp.arange(row_count, dtype=jnp.int32)
    last_query = first_row + row_count - 1
    first_doc = doc_ids[0]
    query_split = query_pairs.reshape(row_count, local_heads, 2, key_width)

    def absorb_block(running, key_block, value_block, doc_block, key_start):
        best, denom, numer = running
        span_len = key_block.shape[0]
        key_pos = key_start + jnp.arange(span_len, dtype=jnp.int32)
        allowed = (key_pos[None, :] <= query_pos[:, None]) & (
            doc_block[None, :] == doc_ids[:, None]
        )
        scores = (
            jnp.einsum(
                "qhmd,khmd->hmqk",
                query_split,
                key_block.reshape(span_len, local_heads, 2, key_width),
                preferred_element_type=jnp.float32,
            )
            * scaling
        )
        scores = jnp.where(allowed, scores, floor_score)
        new_best = jnp.maximum(best, jnp.max(scores, axis=-1))
        weights = jnp.where(allowed, jnp.exp(scores - new_best[..., None]), 0.0)
        fade = jnp.exp(best - new_best)
        denom = denom * fade + jnp.sum(weights, axis=-1)
        numer = numer * fade[..., None] + jnp.einsum(
            "hmqk,khv->hmqv",
            weights.astype(jnp.bfloat16),
            value_block.reshape(span_len, local_heads, value_width),
            preferred_element_type=jnp.float32,
        )
        return (new_best, denom, numer)

    start_best = jnp.full((local_heads, 2, row_count), floor_score, jnp.float32)
    start_denom = jnp.zeros((local_heads, 2, row_count), jnp.float32)
    start_numer = jnp.zeros((local_heads, 2, row_count, value_width), jnp.float32)
    key_piece = lax.all_gather(key_pairs, "sp", axis=0, tiled=True)
    value_piece = lax.all_gather(value_rows, "sp", axis=0, tiled=True)
    doc_piece = lax.all_gather(doc_ids, "sp", axis=0, tiled=True)
    length = key_piece.shape[0]
    span_len = row_count * max(1, 512 // row_count)

    def one_span(span_index, carried):
        offset = span_index * span_len
        key_block = lax.dynamic_slice_in_dim(key_piece, offset, span_len, 0)
        value_block = lax.dynamic_slice_in_dim(value_piece, offset, span_len, 0)
        doc_block = lax.dynamic_slice_in_dim(doc_piece, offset, span_len, 0)
        needed = (offset <= last_query) & (doc_block[span_len - 1] >= first_doc)
        return lax.cond(
            needed,
            lambda held: absorb_block(held, key_block, value_block, doc_block, offset),
            lambda held: held,
            carried,
        )

    best, denom, numer = lax.fori_loop(
        0, length // span_len, one_span, (start_best, start_denom, start_numer)
    )
    heard = numer / denom[..., None]
    contrast = heard[:, 0] - contrast_lambda[:, None, None] * heard[:, 1]
    contrast = (
        contrast
        * lax.rsqrt(jnp.mean(contrast * contrast, axis=-1, keepdims=True) + epsilon)
        * head_gain
    )
    head_out = (
        jnp.transpose(contrast, (1, 0, 2))
        .reshape(row_count, local_heads * value_width)
        .astype(jnp.bfloat16)
    )
    projected = add_columns(out_proj, lax.all_gather(head_out, "tp", axis=1, tiled=True))
    hidden_cols = (stream.astype(jnp.float32) + projected).astype(jnp.bfloat16)
    hidden_rows = lax.all_gather(hidden_cols, "tp", axis=1, tiled=True)
    widened = hidden_rows.astype(jnp.float32)
    normed = (
        widened
        * lax.rsqrt(jnp.mean(widened * widened, axis=-1, keepdims=True) + epsilon)
        * norm_gain
    ).astype(jnp.bfloat16)
    shared_act = (
        jax.nn.silu(jnp.dot(normed, shared_gate, preferred_element_type=jnp.float32))
        * jnp.dot(normed, shared_up, preferred_element_type=jnp.float32)
    ).astype(jnp.bfloat16)
    shared_cols = add_columns(shared_down, lax.all_gather(shared_act, "tp", axis=1, tiled=True))
    expert_count = lax.axis_size("sp")
    route_count = routes.shape[1]
    capacity = 2 * row_count * route_count // expert_count
    flat_routes = routes.reshape(-1)
    hits = (flat_routes[:, None] == jnp.arange(expert_count, dtype=jnp.int32)[None, :]).astype(
        jnp.int32
    )
    position = jnp.sum(jnp.cumsum(hits, axis=0) * hits, axis=1) - 1
    target = flat_routes * capacity + position
    sources = jnp.arange(flat_routes.shape[0], dtype=jnp.int32) // route_count
    owner = jnp.zeros((expert_count * capacity,), jnp.int32).at[target].set(sources)
    outgoing = normed[owner].reshape(expert_count, capacity, normed.shape[1])
    gate_cols = expert_gate[0]
    up_cols = expert_up[0]
    down_cols = expert_down[0]
    slice_width = outgoing.shape[2] // lax.axis_size("tp")
    own_slice = lax.dynamic_slice_in_dim(
        outgoing, lax.axis_index("tp") * slice_width, slice_width, 2
    )
    arrived = lax.all_to_all(own_slice, "sp", split_axis=0, concat_axis=0, tiled=True)
    apply_arrived = lax.all_gather(arrived, "tp", axis=2, tiled=True)
    gated = jnp.einsum("snd,df->snf", apply_arrived, gate_cols, preferred_element_type=jnp.float32)
    lifted = jnp.einsum("snd,df->snf", apply_arrived, up_cols, preferred_element_type=jnp.float32)
    expert_act = (jax.nn.silu(gated) * lifted).astype(jnp.bfloat16)
    expert_out = add_columns(
        down_cols, lax.all_gather(expert_act, "tp", axis=2, tiled=True)
    ).astype(jnp.bfloat16)
    returned = lax.all_to_all(expert_out, "sp", split_axis=0, concat_axis=0, tiled=True)
    flat_back = returned.reshape(expert_count * capacity, returned.shape[2])
    picked = (
        flat_back[target].reshape(row_count, route_count, returned.shape[2]).astype(jnp.float32)
    )
    routed = jnp.sum(picked * route_weights[:, :, None], axis=1)
    return (hidden_cols.astype(jnp.float32) + shared_cols + routed).astype(jnp.bfloat16)


def pair_swap(size, mask):
    return [(i, i ^ mask) for i in range(size)]


def swap(x, axis, mask):
    return lax.ppermute(x, axis, pair_swap(lax.axis_size(axis), mask))


def gather_pieces(own):
    half = own.shape[0] // 2
    one = swap(own, "tp", 1)
    two = swap(own, "tp", 2)
    three = jnp.concatenate([swap(one[:half], "tp", 2), swap(two[half:], "tp", 1)], axis=0)
    return (own, one, two, three)


def vmem(shape=None, index_map=None):
    if shape is None:
        return pl.BlockSpec(memory_space=pltpu.VMEM)
    return pl.BlockSpec(shape, index_map)


def smem():
    return pl.BlockSpec(memory_space=pltpu.SMEM)


def cost(flops, nbytes):
    return pl.CostEstimate(flops=flops, bytes_accessed=nbytes, transcendentals=0)


def params():
    return pltpu.CompilerParams(vmem_limit_bytes=48 * 1024 * 1024)


def fold_kernel(query_ref, key_ref, value_ref, doc_ref, out_ref):
    groups, width, rows = out_ref.shape
    for place, ref in enumerate((query_ref, key_ref, value_ref)):
        turned = ref[...].astype(jnp.float32).T.astype(jnp.bfloat16)
        each = turned.shape[0] // groups
        for group in range(groups):
            out_ref[group, place * each : (place + 1) * each, :] = turned[
                group * each : (group + 1) * each
            ]
    tail = 3 * (query_ref.shape[1] // groups)
    docs = jnp.broadcast_to(doc_ref[...].astype(jnp.bfloat16), (width - tail, rows))
    for group in range(groups):
        out_ref[group, tail:, :] = docs


def attend_kernel(lam_ref, block_ref, gain_ref, out_ref, keys_ref, docs_ref, *, key_width):
    blocks, _, rows = block_ref.shape
    qk = 2 * key_width
    value_width = out_ref.shape[1]
    scaling = key_width ** (-0.5)
    doc_rows = jnp.concatenate(
        [block_ref[b, qk * 2 + value_width :, :][0:1] for b in range(blocks)], axis=0
    ).astype(jnp.float32)
    doc_cols = doc_rows.T
    for b in range(blocks):
        keys_ref[b] = block_ref[b, qk : 2 * qk, :].astype(jnp.float32).T.astype(jnp.bfloat16)
        docs_ref[b] = jnp.broadcast_to(doc_cols[:, b : b + 1], (rows, 128))
    last_docs = doc_rows[:, rows - 1 : rows]
    lows = [
        jnp.sum((last_docs < doc_rows[b : b + 1, 0:1]).astype(jnp.float32)).astype(jnp.int32)
        for b in range(blocks)
    ]
    feature = lax.broadcasted_iota(jnp.int32, (qk, rows), 0)
    key_at = lax.broadcasted_iota(jnp.int32, (rows, rows), 0)
    query_at = lax.broadcasted_iota(jnp.int32, (rows, rows), 1)
    for q in range(blocks):
        turned = block_ref[q, 0:qk, :]
        zero = jnp.zeros_like(turned)
        both = jnp.concatenate(
            [
                jnp.where(feature < key_width, turned, zero),
                jnp.where(feature >= key_width, turned, zero),
            ],
            axis=1,
        )
        query_docs = doc_rows[q : q + 1, :]

        def absorb(k, carried, both=both, query_docs=query_docs, q=q):
            best, denom, numer = carried
            scores = jnp.dot(keys_ref[k], both, preferred_element_type=jnp.float32) * scaling
            key_docs = jnp.concatenate([docs_ref[k]] * (rows // 128), axis=1)
            allowed = (key_docs == query_docs) & (key_at <= query_at + (q - k) * rows)
            scores = jnp.concatenate(
                [
                    jnp.where(allowed, scores[:, :rows], floor_score),
                    jnp.where(allowed, scores[:, rows:], floor_score),
                ],
                axis=1,
            )
            new_best = jnp.maximum(best, jnp.max(scores, axis=0, keepdims=True))
            weights = jnp.exp(scores - new_best)
            fade = jnp.exp(best - new_best)
            denom = denom * fade + jnp.sum(weights, axis=0, keepdims=True)
            numer = numer * fade + jnp.dot(
                block_ref[k, 2 * qk : 2 * qk + value_width, :],
                weights.astype(jnp.bfloat16),
                preferred_element_type=jnp.float32,
            )
            return new_best, denom, numer

        best, denom, numer = lax.fori_loop(
            lows[q],
            q + 1,
            absorb,
            (
                jnp.full((1, 2 * rows), floor_score, jnp.float32),
                jnp.zeros((1, 2 * rows), jnp.float32),
                jnp.zeros((value_width, 2 * rows), jnp.float32),
            ),
        )
        heard = numer / denom
        contrast = heard[:, :rows] - lam_ref[0] * heard[:, rows:]
        mean = jnp.mean(contrast * contrast, axis=0, keepdims=True)
        out_ref[q] = (contrast * lax.rsqrt(mean + epsilon) * gain_ref[...]).astype(jnp.bfloat16)


def project_kernel(order_ref, p0, p1, p2, p3, weight_ref, stream_ref, out_ref):
    total = stream_ref[...].astype(jnp.float32)
    for place, ref in enumerate((p0, p1, p2, p3)):
        total += lax.dot_general(
            ref[...],
            weight_ref[order_ref[place]],
            (((0,), (0,)), ((), ())),
            preferred_element_type=jnp.float32,
        )
    out_ref[...] = total.astype(jnp.bfloat16)


def project(order, pieces, weight, stream):
    rows, cols = stream.shape
    depth = weight.shape[0]
    return pl.pallas_call(
        project_kernel,
        out_shape=jax.ShapeDtypeStruct((rows, cols), jnp.bfloat16),
        in_specs=[smem()] + [vmem()] * 6,
        out_specs=vmem(),
        compiler_params=params(),
        cost_estimate=cost(2 * rows * depth * cols, 2 * depth * (cols + rows)),
        name="project",
    )(order, *pieces, weight.reshape(4, depth // 4, cols), stream)


def hidden_units_kernel(order_ref, p0, p1, p2, p3, gain_ref, gate_ref, up_ref, out_ref, norm_ref):
    @pl.when(pl.program_id(0) == 0)
    def _():
        wide = [ref[...].astype(jnp.float32) for ref in (p0, p1, p2, p3)]
        square = sum(jnp.sum(piece * piece, axis=1, keepdims=True) for piece in wide)
        scale = lax.rsqrt(square / (4 * p0.shape[1]) + epsilon)
        for place, piece in enumerate(wide):
            norm_ref[place] = (piece * scale * gain_ref[order_ref[place]]).astype(jnp.bfloat16)

    gated = jnp.zeros(out_ref.shape, jnp.float32)
    lifted = jnp.zeros(out_ref.shape, jnp.float32)
    for place in range(4):
        gated += jnp.dot(
            norm_ref[place], gate_ref[order_ref[place]], preferred_element_type=jnp.float32
        )
        lifted += jnp.dot(
            norm_ref[place], up_ref[order_ref[place]], preferred_element_type=jnp.float32
        )
    out_ref[...] = (gated / (1.0 + jnp.exp(-gated)) * lifted).astype(jnp.bfloat16)


def hidden_units(order, pieces, gain, gate, up, name):
    rows, width = pieces[0].shape
    depth, cols = gate.shape
    tile = cols // 2
    whole = vmem((rows, width), lambda j: (0, 0))
    strip = vmem((4, width, tile), lambda j: (0, 0, j))
    return pl.pallas_call(
        hidden_units_kernel,
        out_shape=jax.ShapeDtypeStruct((rows, cols), jnp.bfloat16),
        grid=(2,),
        in_specs=[smem(), whole, whole, whole, whole, vmem((4, 1, width), lambda j: (0, 0, 0)), strip, strip],
        out_specs=vmem((rows, tile), lambda j: (0, j)),
        scratch_shapes=[pltpu.VMEM((4, rows, width), jnp.bfloat16)],
        compiler_params=params(),
        cost_estimate=cost(4 * rows * depth * cols, 4 * depth * cols + 2 * rows * depth),
        name=name,
    )(
        order,
        *pieces,
        gain.reshape(4, 1, width),
        gate.reshape(4, width, cols),
        up.reshape(4, width, cols),
    )


def features_kernel(order_ref, p0, p1, p2, p3, down_ref, out_ref):
    total = jnp.zeros(out_ref.shape, jnp.float32)
    for place, ref in enumerate((p0, p1, p2, p3)):
        total += jnp.dot(ref[...], down_ref[order_ref[place]], preferred_element_type=jnp.float32)
    out_ref[...] = total.astype(out_ref.dtype)


def features(order, pieces, down, dtype, name):
    rows, width = pieces[0].shape
    depth, cols = down.shape
    return pl.pallas_call(
        features_kernel,
        out_shape=jax.ShapeDtypeStruct((rows, cols), dtype),
        in_specs=[smem()] + [vmem()] * 5,
        out_specs=vmem(),
        compiler_params=params(),
        cost_estimate=cost(2 * rows * depth * cols, 2 * depth * cols + 2 * rows * depth),
        name=name,
    )(order, *pieces, down.reshape(4, width, cols))


def pack_kernel(expert_ref, routes_ref, rows_ref, out_ref):
    experts, capacity, _ = out_ref.shape
    rows = rows_ref.shape[0]
    earlier = (
        lax.broadcasted_iota(jnp.int32, (rows, rows), 0)
        < lax.broadcasted_iota(jnp.int32, (rows, rows), 1)
    ).astype(jnp.bfloat16)
    routes = routes_ref[...]
    hits = jnp.concatenate(
        [
            jnp.max((routes == expert_ref[place]).astype(jnp.float32), axis=0, keepdims=True)
            for place in range(experts)
        ],
        axis=0,
    )
    ranks = jnp.dot(hits.astype(jnp.bfloat16), earlier, preferred_element_type=jnp.float32)
    ranks = jnp.where(hits > 0, ranks, -1.0).astype(jnp.int32)
    slots = lax.broadcasted_iota(jnp.int32, (capacity, rows), 0)
    held = rows_ref[...]
    for place in range(experts):
        chosen = (slots == ranks[place : place + 1, :]).astype(jnp.bfloat16)
        out_ref[place] = jnp.dot(chosen, held, preferred_element_type=jnp.float32).astype(
            jnp.bfloat16
        )


def pack(experts, routes, rows, capacity):
    count = experts.shape[0]
    return pl.pallas_call(
        pack_kernel,
        out_shape=jax.ShapeDtypeStruct((count, capacity, rows.shape[1]), jnp.bfloat16),
        in_specs=[smem(), vmem(), vmem()],
        out_specs=vmem(),
        compiler_params=params(),
        cost_estimate=cost(2 * count * capacity * rows.size, 4 * count * capacity * rows.shape[1]),
        name="pack",
    )(experts, routes.T, rows)


def combine_kernel(expert_ref, routes_ref, weights_ref, hidden_ref, shared_ref, *refs):
    parts, out_ref = refs[:-1], refs[-1]
    rows = hidden_ref.shape[0]
    capacity = parts[0].shape[0]
    earlier = (
        lax.broadcasted_iota(jnp.int32, (rows, rows), 1)
        < lax.broadcasted_iota(jnp.int32, (rows, rows), 0)
    ).astype(jnp.bfloat16)
    slots = lax.broadcasted_iota(jnp.int32, (rows, capacity), 1)
    routes = routes_ref[...]
    weights = weights_ref[...]
    total = hidden_ref[...].astype(jnp.float32) + shared_ref[...]
    for place, ref in enumerate(parts):
        matches = routes == expert_ref[place]
        hit = jnp.max(matches.astype(jnp.float32), axis=1, keepdims=True)
        share = jnp.sum(jnp.where(matches, weights, 0.0), axis=1, keepdims=True)
        rank = jnp.dot(
            earlier,
            jnp.broadcast_to(hit, (rows, capacity)).astype(jnp.bfloat16),
            preferred_element_type=jnp.float32,
        ).astype(jnp.int32)
        chosen = ((slots == rank) & (hit > 0)).astype(jnp.bfloat16)
        total += share * jnp.dot(chosen, ref[...], preferred_element_type=jnp.float32)
    out_ref[...] = total.astype(jnp.bfloat16)


def combine(experts, routes, weights, hidden, shared, parts):
    rows, cols = hidden.shape
    return pl.pallas_call(
        combine_kernel,
        out_shape=jax.ShapeDtypeStruct((rows, cols), jnp.bfloat16),
        in_specs=[smem()] + [vmem()] * (4 + len(parts)),
        out_specs=vmem(),
        compiler_params=params(),
        cost_estimate=cost(4 * rows * parts[0].size * len(parts), 4 * parts[0].size * len(parts)),
        name="combine",
    )(experts, routes, weights, hidden, shared, *parts)


def swapped_shards(
    query_pairs,
    key_pairs,
    value_rows,
    doc_ids,
    contrast_lambda,
    head_gain,
    stream,
    out_proj,
    norm_gain,
    routes,
    route_weights,
    expert_gate,
    expert_up,
    expert_down,
    shared_gate,
    shared_up,
    shared_down,
):
    rows = query_pairs.shape[0]
    sp_size = lax.axis_size("sp")
    sp_at = lax.axis_index("sp")
    tp_at = lax.axis_index("tp")
    qk = query_pairs.shape[1] // sp_size
    value_width = value_rows.shape[1] // sp_size
    width = 2 * qk + value_width + 16
    order = jnp.bitwise_xor(tp_at, jnp.arange(4, dtype=jnp.int32))
    experts = jnp.bitwise_xor(sp_at, jnp.arange(sp_size, dtype=jnp.int32))

    folded = pl.pallas_call(
        fold_kernel,
        out_shape=jax.ShapeDtypeStruct((sp_size, width, rows), jnp.bfloat16),
        in_specs=[vmem()] * 4,
        out_specs=vmem(),
        compiler_params=params(),
        name="fold",
    )(query_pairs, key_pairs, value_rows, doc_ids.reshape(1, rows))
    blocks = lax.all_to_all(folded, "sp", split_axis=0, concat_axis=0, tiled=True)
    heard = pl.pallas_call(
        functools.partial(attend_kernel, key_width=qk // 2),
        out_shape=jax.ShapeDtypeStruct((sp_size, value_width, rows), jnp.bfloat16),
        in_specs=[smem(), vmem(), vmem()],
        out_specs=vmem(),
        scratch_shapes=[
            pltpu.VMEM((sp_size, rows, qk), jnp.bfloat16),
            pltpu.VMEM((sp_size, rows, 128), jnp.float32),
        ],
        compiler_params=params(),
        cost_estimate=cost(sp_size * sp_size * rows * rows * 128, 2 * blocks.size),
        name="attend",
    )(lax.dynamic_slice_in_dim(contrast_lambda, sp_at, 1, 0), blocks, head_gain[:, None])
    back = lax.all_to_all(heard, "sp", split_axis=0, concat_axis=0, tiled=True)
    head_pieces = gather_pieces(back.reshape(sp_size * value_width, rows))
    hidden = project(order, head_pieces, out_proj, stream)

    capacity = 2 * rows * routes.shape[1] // sp_size
    packed = pack(experts, routes, hidden, capacity)
    shared_pieces = gather_pieces(hidden)
    chunks = []
    for pair in range(0, sp_size, 2):
        first = swap(packed[pair], "sp", pair) if pair else packed[0]
        second = swap(packed[pair + 1], "sp", pair + 1)
        chunks.append(gather_pieces(jnp.concatenate([first, second], axis=0)))
    shared_units = hidden_units(order, shared_pieces, norm_gain, shared_gate, shared_up, "shared_units")
    shared_unit_pieces = gather_pieces(shared_units)
    parts = []
    for at, pieces in enumerate(chunks):
        units = hidden_units(order, pieces, norm_gain, expert_gate[0], expert_up[0], f"units_{at}")
        outs = features(
            order, gather_pieces(units), expert_down[0], jnp.bfloat16, f"features_{at}"
        )
        parts.append(swap(outs[:capacity], "sp", 2 * at) if at else outs[:capacity])
        parts.append(swap(outs[capacity:], "sp", 2 * at + 1))
    shared = features(order, shared_unit_pieces, shared_down, jnp.float32, "shared_features")
    return combine(experts, routes, route_weights, hidden, shared, parts)


def solution(mesh):
    sp_size, tp_size = mesh.shape["sp"], mesh.shape["tp"]

    def body(*arrays):
        heads = arrays[4].shape[0]
        if tp_size == 4 and heads == sp_size and sp_size & (sp_size - 1) == 0:
            return swapped_shards(*arrays)
        return shards(*arrays)

    return jax.shard_map(
        body,
        mesh=mesh,
        in_specs=(
            P("sp", "tp"),
            P("sp", "tp"),
            P("sp", "tp"),
            P("sp"),
            P("tp"),
            P(),
            P("sp", "tp"),
            P(None, "tp"),
            P(),
            P("sp", None),
            P("sp", None),
            P("sp", None, "tp"),
            P("sp", None, "tp"),
            P("sp", None, "tp"),
            P(None, "tp"),
            P(None, "tp"),
            P(None, "tp"),
        ),
        out_specs=P("sp", "tp"),
        check_vma=False,
    )
```

```python
import functools
import math

import jax
import jax.numpy as jnp
from jax import lax
from jax.experimental import pallas as pl
from jax.experimental.pallas import tpu as pltpu

from jax.sharding import PartitionSpec as P

epsilon = 1e-06
floor_score = -1e30


def add_columns(weight_rows, part_block):
    return jnp.dot(part_block, weight_rows, preferred_element_type=jnp.float32)


def shards(
    query_pairs,
    key_pairs,
    value_rows,
    doc_ids,
    contrast_lambda,
    head_gain,
    stream,
    out_proj,
    norm_gain,
    routes,
    route_weights,
    expert_gate,
    expert_up,
    expert_down,
    shared_gate,
    shared_up,
    shared_down,
):
    row_count = query_pairs.shape[0]
    local_heads = contrast_lambda.shape[0]
    key_width = query_pairs.shape[1] // (2 * local_heads)
    value_width = value_rows.shape[1] // local_heads
    scaling = key_width ** (-0.5)
    first_row = lax.axis_index("sp") * row_count
    query_pos = first_row + jnp.arange(row_count, dtype=jnp.int32)
    last_query = first_row + row_count - 1
    first_doc = doc_ids[0]
    query_split = query_pairs.reshape(row_count, local_heads, 2, key_width)

    def absorb_block(running, key_block, value_block, doc_block, key_start):
        best, denom, numer = running
        span_len = key_block.shape[0]
        key_pos = key_start + jnp.arange(span_len, dtype=jnp.int32)
        allowed = (key_pos[None, :] <= query_pos[:, None]) & (
            doc_block[None, :] == doc_ids[:, None]
        )
        scores = (
            jnp.einsum(
                "qhmd,khmd->hmqk",
                query_split,
                key_block.reshape(span_len, local_heads, 2, key_width),
                preferred_element_type=jnp.float32,
            )
            * scaling
        )
        scores = jnp.where(allowed, scores, floor_score)
        new_best = jnp.maximum(best, jnp.max(scores, axis=-1))
        weights = jnp.where(allowed, jnp.exp(scores - new_best[..., None]), 0.0)
        fade = jnp.exp(best - new_best)
        denom = denom * fade + jnp.sum(weights, axis=-1)
        numer = numer * fade[..., None] + jnp.einsum(
            "hmqk,khv->hmqv",
            weights.astype(jnp.bfloat16),
            value_block.reshape(span_len, local_heads, value_width),
            preferred_element_type=jnp.float32,
        )
        return (new_best, denom, numer)

    start_best = jnp.full((local_heads, 2, row_count), floor_score, jnp.float32)
    start_denom = jnp.zeros((local_heads, 2, row_count), jnp.float32)
    start_numer = jnp.zeros((local_heads, 2, row_count, value_width), jnp.float32)
    key_piece = lax.all_gather(key_pairs, "sp", axis=0, tiled=True)
    value_piece = lax.all_gather(value_rows, "sp", axis=0, tiled=True)
    doc_piece = lax.all_gather(doc_ids, "sp", axis=0, tiled=True)
    length = key_piece.shape[0]
    span_len = row_count * max(1, 512 // row_count)

    def one_span(span_index, carried):
        offset = span_index * span_len
        key_block = lax.dynamic_slice_in_dim(key_piece, offset, span_len, 0)
        value_block = lax.dynamic_slice_in_dim(value_piece, offset, span_len, 0)
        doc_block = lax.dynamic_slice_in_dim(doc_piece, offset, span_len, 0)
        needed = (offset <= last_query) & (doc_block[span_len - 1] >= first_doc)
        return lax.cond(
            needed,
            lambda held: absorb_block(held, key_block, value_block, doc_block, offset),
            lambda held: held,
            carried,
        )

    _, denom, numer = lax.fori_loop(
        0, length // span_len, one_span, (start_best, start_denom, start_numer)
    )
    heard = numer / denom[..., None]
    contrast = heard[:, 0] - contrast_lambda[:, None, None] * heard[:, 1]
    contrast = (
        contrast
        * lax.rsqrt(jnp.mean(contrast * contrast, axis=-1, keepdims=True) + epsilon)
        * head_gain
    )
    head_out = (
        jnp.transpose(contrast, (1, 0, 2))
        .reshape(row_count, local_heads * value_width)
        .astype(jnp.bfloat16)
    )
    projected = add_columns(out_proj, lax.all_gather(head_out, "tp", axis=1, tiled=True))
    hidden_cols = (stream.astype(jnp.float32) + projected).astype(jnp.bfloat16)
    hidden_rows = lax.all_gather(hidden_cols, "tp", axis=1, tiled=True)
    widened = hidden_rows.astype(jnp.float32)
    normed = (
        widened
        * lax.rsqrt(jnp.mean(widened * widened, axis=-1, keepdims=True) + epsilon)
        * norm_gain
    ).astype(jnp.bfloat16)
    shared_act = (
        jax.nn.silu(jnp.dot(normed, shared_gate, preferred_element_type=jnp.float32))
        * jnp.dot(normed, shared_up, preferred_element_type=jnp.float32)
    ).astype(jnp.bfloat16)
    shared_cols = add_columns(shared_down, lax.all_gather(shared_act, "tp", axis=1, tiled=True))
    expert_count = lax.axis_size("sp")
    route_count = routes.shape[1]
    capacity = 2 * row_count * route_count // expert_count
    flat_routes = routes.reshape(-1)
    hits = (flat_routes[:, None] == jnp.arange(expert_count, dtype=jnp.int32)[None, :]).astype(
        jnp.int32
    )
    position = jnp.sum(jnp.cumsum(hits, axis=0) * hits, axis=1) - 1
    target = flat_routes * capacity + position
    sources = jnp.arange(flat_routes.shape[0], dtype=jnp.int32) // route_count
    owner = jnp.zeros((expert_count * capacity,), jnp.int32).at[target].set(sources)
    outgoing = normed[owner].reshape(expert_count, capacity, normed.shape[1])
    gate_cols = expert_gate[0]
    up_cols = expert_up[0]
    down_cols = expert_down[0]
    slice_width = outgoing.shape[2] // lax.axis_size("tp")
    own_slice = lax.dynamic_slice_in_dim(
        outgoing, lax.axis_index("tp") * slice_width, slice_width, 2
    )
    arrived = lax.all_to_all(own_slice, "sp", split_axis=0, concat_axis=0, tiled=True)
    apply_arrived = lax.all_gather(arrived, "tp", axis=2, tiled=True)
    gated = jnp.einsum("snd,df->snf", apply_arrived, gate_cols, preferred_element_type=jnp.float32)
    lifted = jnp.einsum("snd,df->snf", apply_arrived, up_cols, preferred_element_type=jnp.float32)
    expert_act = (jax.nn.silu(gated) * lifted).astype(jnp.bfloat16)
    expert_out = add_columns(
        down_cols, lax.all_gather(expert_act, "tp", axis=2, tiled=True)
    ).astype(jnp.bfloat16)
    returned = lax.all_to_all(expert_out, "sp", split_axis=0, concat_axis=0, tiled=True)
    flat_back = returned.reshape(expert_count * capacity, returned.shape[2])
    picked = (
        flat_back[target].reshape(row_count, route_count, returned.shape[2]).astype(jnp.float32)
    )
    routed = jnp.sum(picked * route_weights[:, :, None], axis=1)
    return (hidden_cols.astype(jnp.float32) + shared_cols + routed).astype(jnp.bfloat16)


def pair_swap(size, mask):
    return [(i, i ^ mask) for i in range(size)]


def swap(x, axis, mask):
    return lax.ppermute(x, axis, pair_swap(lax.axis_size(axis), mask))


def gather_pieces(own, relay):
    one = swap(own, "tp", 1)
    two = swap(own, "tp", 2)
    three = swap(one if relay == 2 else two, "tp", relay)
    return (own, one, two, three)


def kernel_call(body, **settings):
    def call(*operands):
        return pl.pallas_call(body, **settings)(*operands)

    return call


def vmem(shape=None, index_map=None):
    if shape is None:
        return pl.BlockSpec(memory_space=pltpu.VMEM)
    return pl.BlockSpec(shape, index_map)


def smem():
    return pl.BlockSpec(memory_space=pltpu.SMEM)


def cost(flops, nbytes):
    return pl.CostEstimate(flops=flops, bytes_accessed=nbytes, transcendentals=0)


def params(mebibytes=48):
    return pltpu.CompilerParams(vmem_limit_bytes=mebibytes * 1024 * 1024)


def fold_kernel(query_ref, key_ref, value_ref, doc_ref, out_ref):
    groups, width, rows = out_ref.shape
    for place, ref in enumerate((query_ref, key_ref, value_ref)):
        turned = ref[...].astype(jnp.float32).T.astype(jnp.bfloat16)
        each = turned.shape[0] // groups
        for group in range(groups):
            out_ref[group, place * each : (place + 1) * each, :] = turned[
                group * each : (group + 1) * each
            ]
    tail = 3 * (query_ref.shape[1] // groups)
    docs = jnp.broadcast_to(doc_ref[...].astype(jnp.bfloat16), (width - tail, rows))
    for group in range(groups):
        out_ref[group, tail:, :] = docs


def attend_kernel(
    lam_ref, block_ref, gain_ref, out_ref, keys_ref, cols_ref, rows_ref, low_ref, *, key_width
):
    blocks, _, rows = block_ref.shape
    qk = 2 * key_width
    value_width = out_ref.shape[1]
    power = key_width ** (-0.5) * math.log2(math.e)
    doc_rows = jnp.concatenate(
        [block_ref[b, qk * 2 + value_width :, :][0:1] for b in range(blocks)], axis=0
    ).astype(jnp.float32)
    doc_cols = doc_rows.T
    first_docs, last_docs = doc_rows[:, 0:1], doc_rows[:, rows - 1 : rows]
    for b in range(blocks):
        keys_ref[b] = block_ref[b, qk : 2 * qk, :].astype(jnp.float32).T.astype(jnp.bfloat16)
        cols_ref[b] = jnp.broadcast_to(doc_cols[:, b : b + 1], (rows, 128))
        rows_ref[b] = jnp.broadcast_to(doc_rows[b : b + 1], (8, rows))
        for at, earlier in enumerate(
            (last_docs < first_docs[b : b + 1], first_docs < last_docs[b : b + 1])
        ):
            low_ref[at, b] = jnp.sum(earlier.astype(jnp.float32)).astype(jnp.int32)
    feature = lax.broadcasted_iota(jnp.int32, (qk, rows), 0)

    def one_block(q, _):
        turned = block_ref[q, 0:qk, :]
        zero = jnp.zeros_like(turned)
        halves = (
            jnp.where(feature < key_width, turned, zero),
            jnp.where(feature >= key_width, turned, zero),
        )
        query_docs = rows_ref[q][0:1]

        def absorb(k, carried, mask):
            keys = keys_ref[k]
            values = block_ref[k, 2 * qk : 2 * qk + value_width, :]
            if mask:
                allowed = jnp.concatenate([cols_ref[k]] * (rows // 128), axis=1) == query_docs
                if mask == "diagonal":
                    allowed &= lax.broadcasted_iota(
                        jnp.int32, (rows, rows), 0
                    ) <= lax.broadcasted_iota(jnp.int32, (rows, rows), 1)
            after = []
            raw = [jnp.dot(keys, half, preferred_element_type=jnp.float32) for half in halves]
            for scores, (best, denom, numer) in zip(raw, carried):
                if mask:
                    scores = jnp.where(allowed, scores, floor_score)
                new_best = jnp.maximum(best, jnp.max(scores, axis=0, keepdims=True))
                weights = jnp.exp2((scores - new_best) * power)
                fade = jnp.exp2((best - new_best) * power)
                denom = denom * fade + jnp.sum(weights, axis=0, keepdims=True)
                numer = numer * fade + jnp.dot(
                    values, weights.astype(jnp.bfloat16), preferred_element_type=jnp.float32
                )
                after.append((new_best, denom, numer))
            return tuple(after)

        start = (
            jnp.full((1, rows), floor_score, jnp.float32),
            jnp.zeros((1, rows), jnp.float32),
            jnp.zeros((value_width, rows), jnp.float32),
        )
        full = jnp.minimum(low_ref[1, q], q)
        carried = (start, start)
        carried = lax.fori_loop(low_ref[0, q], full, lambda k, c: absorb(k, c, "document"), carried)
        carried = lax.fori_loop(full, q, lambda k, c: absorb(k, c, None), carried)
        heard = [numer / denom for _, denom, numer in absorb(q, carried, "diagonal")]
        contrast = heard[0] - lam_ref[0] * heard[1]
        mean = jnp.mean(contrast * contrast, axis=0, keepdims=True)
        out_ref[q] = (contrast * lax.rsqrt(mean + epsilon) * gain_ref[...]).astype(jnp.bfloat16)
        return 0

    lax.fori_loop(0, blocks, one_block, 0)


def project_kernel(order_ref, p0, p1, p2, p3, weight_ref, stream_ref, out_ref):
    total = stream_ref[...].astype(jnp.float32)
    for place, ref in enumerate((p0, p1, p2, p3)):
        total += lax.dot_general(
            ref[...],
            weight_ref[order_ref[place]],
            (((0,), (0,)), ((), ())),
            preferred_element_type=jnp.float32,
        )
    out_ref[...] = total.astype(jnp.bfloat16)


def project(order, pieces, weight, stream):
    rows, cols = stream.shape
    depth = weight.shape[0]
    tile = cols // 2
    piece = vmem((depth // 4, rows), lambda j: (0, 0))
    strip = vmem((rows, tile), lambda j: (0, j))
    return kernel_call(
        project_kernel,
        out_shape=jax.ShapeDtypeStruct((rows, cols), jnp.bfloat16),
        grid=(2,),
        in_specs=[smem()] + [piece] * 4 + [vmem((4, depth // 4, tile), lambda j: (0, 0, j)), strip],
        out_specs=strip,
        compiler_params=params(60),
        cost_estimate=cost(2 * rows * depth * cols, 2 * depth * (cols + rows)),
    )(order, *pieces, weight.reshape(4, depth // 4, cols), stream)


def hidden_units_kernel(order_ref, p0, p1, p2, p3, gain_ref, gate_ref, up_ref, out_ref, norm_ref):
    @pl.when(pl.program_id(0) == 0)
    def _():
        wide = [ref[...].astype(jnp.float32) for ref in (p0, p1, p2, p3)]
        square = sum(jnp.sum(piece * piece, axis=1, keepdims=True) for piece in wide)
        scale = lax.rsqrt(square / (4 * p0.shape[1]) + epsilon)
        for place, piece in enumerate(wide):
            norm_ref[place] = (piece * scale * gain_ref[order_ref[place]]).astype(jnp.bfloat16)

    gated = jnp.zeros(out_ref.shape, jnp.float32)
    lifted = jnp.zeros(out_ref.shape, jnp.float32)
    for place in range(4):
        gated += jnp.dot(
            norm_ref[place], gate_ref[order_ref[place]], preferred_element_type=jnp.float32
        )
        lifted += jnp.dot(
            norm_ref[place], up_ref[order_ref[place]], preferred_element_type=jnp.float32
        )
    out_ref[...] = (gated / (1.0 + jnp.exp(-gated)) * lifted).astype(jnp.bfloat16)


def hidden_units(order, pieces, gain, gate, up):
    rows, width = pieces[0].shape
    depth, cols = gate.shape
    tile = cols // 2
    whole = vmem((rows, width), lambda j: (0, 0))
    strip = vmem((4, width, tile), lambda j: (0, 0, j))
    return kernel_call(
        hidden_units_kernel,
        out_shape=jax.ShapeDtypeStruct((rows, cols), jnp.bfloat16),
        grid=(2,),
        in_specs=[smem(), whole, whole, whole, whole, vmem((4, 1, width), lambda j: (0, 0, 0)), strip, strip],
        out_specs=vmem((rows, tile), lambda j: (0, j)),
        scratch_shapes=[pltpu.VMEM((4, rows, width), jnp.bfloat16)],
        compiler_params=params(24),
        cost_estimate=cost(4 * rows * depth * cols, 4 * depth * cols + 2 * rows * depth),
    )(
        order,
        *pieces,
        gain.reshape(4, 1, width),
        gate.reshape(4, width, cols),
        up.reshape(4, width, cols),
    )


def features_kernel(order_ref, p0, p1, p2, p3, down_ref, out_ref):
    total = jnp.zeros(out_ref.shape, jnp.float32)
    for place, ref in enumerate((p0, p1, p2, p3)):
        total += jnp.dot(ref[...], down_ref[order_ref[place]], preferred_element_type=jnp.float32)
    out_ref[...] = total.astype(out_ref.dtype)


def features(order, pieces, down, dtype):
    rows, width = pieces[0].shape
    depth, cols = down.shape
    return kernel_call(
        features_kernel,
        out_shape=jax.ShapeDtypeStruct((rows, cols), dtype),
        in_specs=[smem()] + [vmem()] * 5,
        out_specs=vmem(),
        compiler_params=params(24),
        cost_estimate=cost(2 * rows * depth * cols, 2 * depth * cols + 2 * rows * depth),
    )(order, *pieces, down.reshape(4, width, cols))


def pack_kernel(expert_ref, own_routes_ref, near_routes_ref, own_ref, near_ref, *outs):
    experts = len(outs)
    capacity = outs[0].shape[0] // 2
    rows = own_ref.shape[0]
    earlier = (
        lax.broadcasted_iota(jnp.int32, (rows, rows), 0)
        < lax.broadcasted_iota(jnp.int32, (rows, rows), 1)
    ).astype(jnp.bfloat16)
    slots = lax.broadcasted_iota(jnp.int32, (capacity, rows), 0)
    for half, (routes_ref, rows_ref) in enumerate(
        ((own_routes_ref, own_ref), (near_routes_ref, near_ref))
    ):
        routes = routes_ref[...]
        hits = jnp.concatenate(
            [
                jnp.max((routes == expert_ref[place]).astype(jnp.float32), axis=0, keepdims=True)
                for place in range(experts)
            ],
            axis=0,
        )
        ranks = jnp.dot(hits.astype(jnp.bfloat16), earlier, preferred_element_type=jnp.float32)
        ranks = jnp.where(hits > 0, ranks, -1.0).astype(jnp.int32)
        held = rows_ref[...]
        for place in range(experts):
            chosen = (slots == ranks[place : place + 1, :]).astype(jnp.bfloat16)
            outs[place][half * capacity : (half + 1) * capacity, :] = jnp.dot(
                chosen, held, preferred_element_type=jnp.float32
            ).astype(jnp.bfloat16)


def pack(experts, own_routes, near_routes, own, near, capacity):
    count = experts.shape[0]
    cols = own.shape[1]
    return kernel_call(
        pack_kernel,
        out_shape=[jax.ShapeDtypeStruct((2 * capacity, cols), jnp.bfloat16)] * count,
        in_specs=[smem()] + [vmem()] * 4,
        out_specs=[vmem()] * count,
        compiler_params=params(),
        cost_estimate=cost(4 * count * capacity * own.size, 8 * count * capacity * cols),
    )(experts, own_routes, near_routes, own, near)


def pack_near_kernel(expert_ref, own_routes_ref, near_routes_ref, *refs):
    pieces, outs = refs[:8], refs[8:]
    capacity = outs[0].shape[0] // 2
    rows = pieces[0].shape[0]
    earlier = (
        lax.broadcasted_iota(jnp.int32, (rows, rows), 0)
        < lax.broadcasted_iota(jnp.int32, (rows, rows), 1)
    ).astype(jnp.bfloat16)
    slots = lax.broadcasted_iota(jnp.int32, (capacity, rows), 0)
    for half, routes_ref in enumerate((own_routes_ref, near_routes_ref)):
        matches = (routes_ref[...] == expert_ref[0]).astype(jnp.float32)
        hit = jnp.max(matches, axis=0, keepdims=True)
        ranks = jnp.dot(
            jnp.broadcast_to(hit, (8, rows)).astype(jnp.bfloat16),
            earlier,
            preferred_element_type=jnp.float32,
        )[0:1]
        ranks = jnp.where(hit > 0, ranks, -1.0).astype(jnp.int32)
        chosen = (slots == ranks).astype(jnp.bfloat16)
        for place, out in enumerate(outs):
            out[half * capacity : (half + 1) * capacity, :] = jnp.dot(
                chosen, pieces[4 * half + place][...], preferred_element_type=jnp.float32
            ).astype(jnp.bfloat16)


def pack_near(experts, own_routes, near_routes, own, near, capacity):
    cols = own[0].shape[1]
    return kernel_call(
        pack_near_kernel,
        out_shape=[jax.ShapeDtypeStruct((2 * capacity, cols), jnp.bfloat16)] * 4,
        in_specs=[smem()] + [vmem()] * 10,
        out_specs=[vmem()] * 4,
        compiler_params=params(),
        cost_estimate=cost(16 * capacity * own[0].size, 16 * own[0].size),
    )(experts, own_routes, near_routes, *own, *near)


def spread_kernel(expert_ref, routes_ref, weights_ref, *refs, half):
    parts, out_ref = refs[:-1], refs[-1]
    rows = routes_ref.shape[0]
    capacity = parts[0].shape[0] // 2
    earlier = (
        lax.broadcasted_iota(jnp.int32, (rows, rows), 1)
        < lax.broadcasted_iota(jnp.int32, (rows, rows), 0)
    ).astype(jnp.bfloat16)
    slots = lax.broadcasted_iota(jnp.int32, (rows, capacity), 1)
    routes = routes_ref[...]
    weights = weights_ref[...]
    total = jnp.zeros(out_ref.shape, jnp.float32)
    for place, ref in enumerate(parts):
        matches = routes == expert_ref[place]
        hit = jnp.max(matches.astype(jnp.float32), axis=1, keepdims=True)
        share = jnp.sum(jnp.where(matches, weights, 0.0), axis=1, keepdims=True)
        rank = jnp.dot(
            earlier,
            jnp.broadcast_to(hit, (rows, capacity)).astype(jnp.bfloat16),
            preferred_element_type=jnp.float32,
        ).astype(jnp.int32)
        chosen = ((slots == rank) & (hit > 0)).astype(jnp.bfloat16)
        total += share * jnp.dot(
            chosen,
            ref[half * capacity : (half + 1) * capacity, :],
            preferred_element_type=jnp.float32,
        )
    out_ref[...] = total


def spread(experts, routes, weights, parts, half):
    rows = routes.shape[0]
    capacity, cols = parts[0].shape[0] // 2, parts[0].shape[1]
    return kernel_call(
        functools.partial(spread_kernel, half=half),
        out_shape=jax.ShapeDtypeStruct((rows, cols), jnp.float32),
        in_specs=[smem()] + [vmem()] * (2 + len(parts)),
        out_specs=vmem(),
        compiler_params=params(),
        cost_estimate=cost(4 * rows * capacity * cols * len(parts), 4 * capacity * cols * len(parts)),
    )(experts, routes, weights, *parts)


def finish_kernel(order_ref, p0, p1, p2, p3, down_ref, hidden_ref, own_ref, near_ref, out_ref):
    total = hidden_ref[...].astype(jnp.float32) + own_ref[...] + near_ref[...]
    for place, ref in enumerate((p0, p1, p2, p3)):
        total += jnp.dot(ref[...], down_ref[order_ref[place]], preferred_element_type=jnp.float32)
    out_ref[...] = total.astype(jnp.bfloat16)


def finish(order, pieces, down, hidden, own, near):
    rows, width = pieces[0].shape
    depth, cols = down.shape
    return kernel_call(
        finish_kernel,
        out_shape=jax.ShapeDtypeStruct((rows, cols), jnp.bfloat16),
        in_specs=[smem()] + [vmem()] * 8,
        out_specs=vmem(),
        compiler_params=params(24),
        cost_estimate=cost(2 * rows * depth * cols, 2 * depth * cols + 2 * rows * depth),
    )(order, *pieces, down.reshape(4, width, cols), hidden, own, near)


def swapped_shards(
    query_pairs,
    key_pairs,
    value_rows,
    doc_ids,
    contrast_lambda,
    head_gain,
    stream,
    out_proj,
    norm_gain,
    routes,
    route_weights,
    expert_gate,
    expert_up,
    expert_down,
    shared_gate,
    shared_up,
    shared_down,
):
    rows = query_pairs.shape[0]
    sp_size = lax.axis_size("sp")
    sp_at = lax.axis_index("sp")
    tp_at = lax.axis_index("tp")
    qk = query_pairs.shape[1] // sp_size
    value_width = value_rows.shape[1] // sp_size
    width = 2 * qk + value_width + 8
    order = jnp.bitwise_xor(tp_at, jnp.arange(4, dtype=jnp.int32))
    experts = jnp.bitwise_xor(sp_at, 2 * jnp.arange(sp_size // 2, dtype=jnp.int32))

    folded = kernel_call(
        fold_kernel,
        out_shape=jax.ShapeDtypeStruct((sp_size, width, rows), jnp.bfloat16),
        in_specs=[vmem()] * 4,
        out_specs=vmem(),
    )(query_pairs, key_pairs, value_rows, doc_ids.reshape(1, rows))
    blocks = lax.all_to_all(folded, "sp", split_axis=0, concat_axis=0, tiled=True)
    heard = kernel_call(
        functools.partial(attend_kernel, key_width=qk // 2),
        out_shape=jax.ShapeDtypeStruct((sp_size, value_width, rows), jnp.bfloat16),
        in_specs=[smem(), vmem(), vmem()],
        out_specs=vmem(),
        scratch_shapes=[
            pltpu.VMEM((sp_size, rows, qk), jnp.bfloat16),
            pltpu.VMEM((sp_size, rows, 128), jnp.float32),
            pltpu.VMEM((sp_size, 8, rows), jnp.float32),
            pltpu.SMEM((2, sp_size), jnp.int32),
        ],
        compiler_params=params(),
        cost_estimate=cost(sp_size * sp_size * rows * rows * 128, 2 * blocks.size),
    )(lax.dynamic_slice_in_dim(contrast_lambda, sp_at, 1, 0), blocks, head_gain[:, None])
    back = lax.all_to_all(heard, "sp", split_axis=0, concat_axis=0, tiled=True)
    near_routes = swap(routes, "sp", 1)
    near_weights = swap(route_weights, "sp", 1)
    head_pieces = gather_pieces(back.reshape(sp_size * value_width, rows), 1)
    hidden = project(order, head_pieces, out_proj, stream)

    capacity = 2 * rows * routes.shape[1] // sp_size
    near_hidden = swap(hidden, "sp", 1)
    turned, near_turned = routes.T, near_routes.T
    packed = pack(experts[1:], turned, near_turned, hidden, near_hidden, capacity)
    shared_pieces = gather_pieces(hidden, 1)
    near_pieces = [near_hidden]
    for at in (1, 2, 3):
        near_pieces.append(swap(shared_pieces[at], "sp", 1))
    shared_units = hidden_units(order, shared_pieces, norm_gain, shared_gate, shared_up)
    parts = []
    for at in range(sp_size // 2):
        if at:
            relay = (1, 1, 2, 2)[at]
            held = swap(packed[at - 1], "sp", 2 * at)
            pieces = gather_pieces(held, relay)
        else:
            pieces = pack_near(experts, turned, near_turned, shared_pieces, near_pieces, capacity)
        units = hidden_units(order, pieces, norm_gain, expert_gate[0], expert_up[0])
        unit_pieces = gather_pieces(units, (2, 2, 1, 1)[at])
        outs = features(order, unit_pieces, expert_down[0], jnp.bfloat16)
        parts.append(swap(outs, "sp", 2 * at) if at else outs)
    for_near = spread(experts, near_routes, near_weights, parts, 1)
    for_own = spread(experts, routes, route_weights, parts, 0)
    shared_unit_pieces = gather_pieces(shared_units, 1)
    near_sum = swap(for_near, "sp", 1)
    return finish(order, shared_unit_pieces, shared_down, hidden, for_own, near_sum)


def solution(mesh):
    sp_size, tp_size = mesh.shape["sp"], mesh.shape["tp"]

    swapped = tp_size == 4 and sp_size == 8

    def body(*arrays):
        if swapped and arrays[4].shape[0] == sp_size:
            return swapped_shards(*arrays)
        return shards(*arrays)

    return jax.shard_map(
        body,
        mesh=mesh,
        in_specs=(
            P("sp", "tp"),
            P("sp", "tp"),
            P("sp", "tp"),
            P("sp"),
            P("tp"),
            P(),
            P("sp", "tp"),
            P(None, "tp"),
            P(),
            P("sp", None),
            P("sp", None),
            P("sp", None, "tp"),
            P("sp", None, "tp"),
            P("sp", None, "tp"),
            P(None, "tp"),
            P(None, "tp"),
            P(None, "tp"),
        ),
        out_specs=P("sp", "tp"),
        check_vma=False,
    )
```

```python
import functools
import math

import jax
import jax.numpy as jnp
from jax import lax
from jax.experimental import pallas as pl
from jax.experimental.pallas import tpu as pltpu

from jax.sharding import PartitionSpec as P

epsilon = 1e-06
floor_score = -1e30


def add_columns(weight_rows, part_block):
    return jnp.dot(part_block, weight_rows, preferred_element_type=jnp.float32)


def shards(
    query_pairs,
    key_pairs,
    value_rows,
    doc_ids,
    contrast_lambda,
    head_gain,
    stream,
    out_proj,
    norm_gain,
    routes,
    route_weights,
    expert_gate,
    expert_up,
    expert_down,
    shared_gate,
    shared_up,
    shared_down,
):
    row_count = query_pairs.shape[0]
    local_heads = contrast_lambda.shape[0]
    key_width = query_pairs.shape[1] // (2 * local_heads)
    value_width = value_rows.shape[1] // local_heads
    scaling = key_width ** (-0.5)
    first_row = lax.axis_index("sp") * row_count
    query_pos = first_row + jnp.arange(row_count, dtype=jnp.int32)
    last_query = first_row + row_count - 1
    first_doc = doc_ids[0]
    query_split = query_pairs.reshape(row_count, local_heads, 2, key_width)

    def absorb_block(running, key_block, value_block, doc_block, key_start):
        best, denom, numer = running
        span_len = key_block.shape[0]
        key_pos = key_start + jnp.arange(span_len, dtype=jnp.int32)
        allowed = (key_pos[None, :] <= query_pos[:, None]) & (
            doc_block[None, :] == doc_ids[:, None]
        )
        scores = (
            jnp.einsum(
                "qhmd,khmd->hmqk",
                query_split,
                key_block.reshape(span_len, local_heads, 2, key_width),
                preferred_element_type=jnp.float32,
            )
            * scaling
        )
        scores = jnp.where(allowed, scores, floor_score)
        new_best = jnp.maximum(best, jnp.max(scores, axis=-1))
        weights = jnp.where(allowed, jnp.exp(scores - new_best[..., None]), 0.0)
        fade = jnp.exp(best - new_best)
        denom = denom * fade + jnp.sum(weights, axis=-1)
        numer = numer * fade[..., None] + jnp.einsum(
            "hmqk,khv->hmqv",
            weights.astype(jnp.bfloat16),
            value_block.reshape(span_len, local_heads, value_width),
            preferred_element_type=jnp.float32,
        )
        return (new_best, denom, numer)

    start_best = jnp.full((local_heads, 2, row_count), floor_score, jnp.float32)
    start_denom = jnp.zeros((local_heads, 2, row_count), jnp.float32)
    start_numer = jnp.zeros((local_heads, 2, row_count, value_width), jnp.float32)
    key_piece = lax.all_gather(key_pairs, "sp", axis=0, tiled=True)
    value_piece = lax.all_gather(value_rows, "sp", axis=0, tiled=True)
    doc_piece = lax.all_gather(doc_ids, "sp", axis=0, tiled=True)
    length = key_piece.shape[0]
    span_len = row_count * max(1, 512 // row_count)

    def one_span(span_index, carried):
        offset = span_index * span_len
        key_block = lax.dynamic_slice_in_dim(key_piece, offset, span_len, 0)
        value_block = lax.dynamic_slice_in_dim(value_piece, offset, span_len, 0)
        doc_block = lax.dynamic_slice_in_dim(doc_piece, offset, span_len, 0)
        needed = (offset <= last_query) & (doc_block[span_len - 1] >= first_doc)
        return lax.cond(
            needed,
            lambda held: absorb_block(held, key_block, value_block, doc_block, offset),
            lambda held: held,
            carried,
        )

    _, denom, numer = lax.fori_loop(
        0, length // span_len, one_span, (start_best, start_denom, start_numer)
    )
    heard = numer / denom[..., None]
    contrast = heard[:, 0] - contrast_lambda[:, None, None] * heard[:, 1]
    contrast = (
        contrast
        * lax.rsqrt(jnp.mean(contrast * contrast, axis=-1, keepdims=True) + epsilon)
        * head_gain
    )
    head_out = (
        jnp.transpose(contrast, (1, 0, 2))
        .reshape(row_count, local_heads * value_width)
        .astype(jnp.bfloat16)
    )
    projected = add_columns(out_proj, lax.all_gather(head_out, "tp", axis=1, tiled=True))
    hidden_cols = (stream.astype(jnp.float32) + projected).astype(jnp.bfloat16)
    hidden_rows = lax.all_gather(hidden_cols, "tp", axis=1, tiled=True)
    widened = hidden_rows.astype(jnp.float32)
    normed = (
        widened
        * lax.rsqrt(jnp.mean(widened * widened, axis=-1, keepdims=True) + epsilon)
        * norm_gain
    ).astype(jnp.bfloat16)
    shared_act = (
        jax.nn.silu(jnp.dot(normed, shared_gate, preferred_element_type=jnp.float32))
        * jnp.dot(normed, shared_up, preferred_element_type=jnp.float32)
    ).astype(jnp.bfloat16)
    shared_cols = add_columns(shared_down, lax.all_gather(shared_act, "tp", axis=1, tiled=True))
    expert_count = lax.axis_size("sp")
    route_count = routes.shape[1]
    capacity = 2 * row_count * route_count // expert_count
    flat_routes = routes.reshape(-1)
    hits = (flat_routes[:, None] == jnp.arange(expert_count, dtype=jnp.int32)[None, :]).astype(
        jnp.int32
    )
    position = jnp.sum(jnp.cumsum(hits, axis=0) * hits, axis=1) - 1
    target = flat_routes * capacity + position
    sources = jnp.arange(flat_routes.shape[0], dtype=jnp.int32) // route_count
    owner = jnp.zeros((expert_count * capacity,), jnp.int32).at[target].set(sources)
    outgoing = normed[owner].reshape(expert_count, capacity, normed.shape[1])
    gate_cols = expert_gate[0]
    up_cols = expert_up[0]
    down_cols = expert_down[0]
    slice_width = outgoing.shape[2] // lax.axis_size("tp")
    own_slice = lax.dynamic_slice_in_dim(
        outgoing, lax.axis_index("tp") * slice_width, slice_width, 2
    )
    arrived = lax.all_to_all(own_slice, "sp", split_axis=0, concat_axis=0, tiled=True)
    apply_arrived = lax.all_gather(arrived, "tp", axis=2, tiled=True)
    gated = jnp.einsum("snd,df->snf", apply_arrived, gate_cols, preferred_element_type=jnp.float32)
    lifted = jnp.einsum("snd,df->snf", apply_arrived, up_cols, preferred_element_type=jnp.float32)
    expert_act = (jax.nn.silu(gated) * lifted).astype(jnp.bfloat16)
    expert_out = add_columns(
        down_cols, lax.all_gather(expert_act, "tp", axis=2, tiled=True)
    ).astype(jnp.bfloat16)
    returned = lax.all_to_all(expert_out, "sp", split_axis=0, concat_axis=0, tiled=True)
    flat_back = returned.reshape(expert_count * capacity, returned.shape[2])
    picked = (
        flat_back[target].reshape(row_count, route_count, returned.shape[2]).astype(jnp.float32)
    )
    routed = jnp.sum(picked * route_weights[:, :, None], axis=1)
    return (hidden_cols.astype(jnp.float32) + shared_cols + routed).astype(jnp.bfloat16)


def pair_swap(size, mask):
    return [(i, i ^ mask) for i in range(size)]


def swap(x, axis, mask):
    return lax.ppermute(x, axis, pair_swap(lax.axis_size(axis), mask))


def gather_pieces(own, relay):
    one = swap(own, "tp", 1)
    two = swap(own, "tp", 2)
    three = swap(one if relay == 2 else two, "tp", relay)
    return (own, one, two, three)


def kernel_call(body, **settings):
    def call(*operands):
        return pl.pallas_call(body, **settings)(*operands)

    return call


def vmem(shape=None, index_map=None):
    if shape is None:
        return pl.BlockSpec(memory_space=pltpu.VMEM)
    return pl.BlockSpec(shape, index_map)


def smem():
    return pl.BlockSpec(memory_space=pltpu.SMEM)


def cost(flops, nbytes):
    return pl.CostEstimate(flops=flops, bytes_accessed=nbytes, transcendentals=0)


def params(mebibytes=48):
    return pltpu.CompilerParams(vmem_limit_bytes=mebibytes * 1024 * 1024)


def fold_kernel(query_ref, key_ref, value_ref, doc_ref, out_ref):
    groups, width, rows = out_ref.shape
    for place, ref in enumerate((query_ref, key_ref, value_ref)):
        turned = ref[...].astype(jnp.float32).T.astype(jnp.bfloat16)
        each = turned.shape[0] // groups
        for group in range(groups):
            out_ref[group, place * each : (place + 1) * each, :] = turned[
                group * each : (group + 1) * each
            ]
    tail = 3 * (query_ref.shape[1] // groups)
    docs = jnp.broadcast_to(doc_ref[...].astype(jnp.bfloat16), (width - tail, rows))
    for group in range(groups):
        out_ref[group, tail:, :] = docs


def attend_kernel(
    lam_ref, block_ref, gain_ref, out_ref, keys_ref, cols_ref, rows_ref, low_ref, *, key_width
):
    blocks, _, rows = block_ref.shape
    qk = 2 * key_width
    value_width = out_ref.shape[1]
    power = key_width ** (-0.5) * math.log2(math.e)
    doc_rows = jnp.concatenate(
        [block_ref[b, qk * 2 + value_width :, :][0:1] for b in range(blocks)], axis=0
    ).astype(jnp.float32)
    doc_cols = doc_rows.T
    first_docs, last_docs = doc_rows[:, 0:1], doc_rows[:, rows - 1 : rows]
    for b in range(blocks):
        turned = block_ref[b, qk : 2 * qk, :].astype(jnp.float32).T
        keys_ref[b * rows : (b + 1) * rows, :] = turned.astype(jnp.bfloat16)
        cols_ref[b] = jnp.broadcast_to(doc_cols[:, b : b + 1], (rows, 128))
        rows_ref[b] = jnp.broadcast_to(doc_rows[b : b + 1], (8, rows))
        earlier = (last_docs < first_docs[b : b + 1]).astype(jnp.float32)
        low_ref[b] = jnp.sum(earlier).astype(jnp.int32)
    feature = lax.broadcasted_iota(jnp.int32, (qk, rows), 0)

    def one_block(q, _):
        turned = block_ref[q, 0:qk, :]
        zero = jnp.zeros_like(turned)
        halves = (
            jnp.where(feature < key_width, turned, zero),
            jnp.where(feature >= key_width, turned, zero),
        )
        query_docs = rows_ref[q][0:1]

        def absorb(k, carried, span):
            keys = keys_ref[pl.ds(pl.multiple_of(k * rows, rows), span * rows), :]
            docs = jnp.concatenate([cols_ref[k + b] for b in range(span)], axis=0)
            allowed = jnp.concatenate([docs] * (rows // 128), axis=1) == query_docs
            ahead = lax.broadcasted_iota(
                jnp.int32, (span * rows, rows), 0
            ) - lax.broadcasted_iota(jnp.int32, (span * rows, rows), 1)
            allowed &= ahead <= (q - k) * rows
            after = []
            raw = [jnp.dot(keys, half, preferred_element_type=jnp.float32) for half in halves]
            for scores, (best, denom, numer) in zip(raw, carried):
                scores = jnp.where(allowed, scores, floor_score)
                new_best = jnp.maximum(best, jnp.max(scores, axis=0, keepdims=True))
                weights = jnp.exp2((scores - new_best) * power)
                fade = jnp.exp2((best - new_best) * power)
                denom = denom * fade + jnp.sum(weights, axis=0, keepdims=True)
                rounded = weights.astype(jnp.bfloat16)
                numer = numer * fade
                for b in range(span):
                    numer += jnp.dot(
                        block_ref[k + b, 2 * qk : 2 * qk + value_width, :],
                        rounded[b * rows : (b + 1) * rows],
                        preferred_element_type=jnp.float32,
                    )
                after.append((new_best, denom, numer))
            return tuple(after)

        start = (
            jnp.full((1, rows), floor_score, jnp.float32),
            jnp.zeros((1, rows), jnp.float32),
            jnp.zeros((value_width, rows), jnp.float32),
        )
        low = low_ref[q]
        odd = lax.rem(q + 1 - low, 2)
        carried = lax.fori_loop(low, low + odd, lambda k, c: absorb(k, c, 1), (start, start))
        carried = lax.fori_loop(
            0,
            lax.div(q + 1 - low, 2),
            lambda step, c: absorb(low + odd + 2 * step, c, 2),
            carried,
        )
        heard = [numer / denom for _, denom, numer in carried]
        contrast = heard[0] - lam_ref[0] * heard[1]
        mean = jnp.mean(contrast * contrast, axis=0, keepdims=True)
        out_ref[q] = (contrast * lax.rsqrt(mean + epsilon) * gain_ref[...]).astype(jnp.bfloat16)
        return 0

    lax.fori_loop(0, blocks, one_block, 0)


def project_kernel(order_ref, *refs, first):
    pieces, (weight_ref, base_ref, out_ref) = refs[:-3], refs[-3:]
    total = base_ref[...].astype(jnp.float32)
    for place, ref in enumerate(pieces):
        total += lax.dot_general(
            ref[...],
            weight_ref[order_ref[first + place]],
            (((0,), (0,)), ((), ())),
            preferred_element_type=jnp.float32,
        )
    out_ref[...] = total.astype(out_ref.dtype)


def project(order, pieces, weight, stream):
    rows, cols = stream.shape
    depth = weight.shape[0] // 4
    weight = weight.reshape(4, depth, cols)

    def add(base, held, first, dtype):
        return kernel_call(
            functools.partial(project_kernel, first=first),
            out_shape=jax.ShapeDtypeStruct((rows, cols), dtype),
            in_specs=[smem()] + [vmem()] * (2 + len(held)),
            out_specs=vmem(),
            compiler_params=params(32),
            cost_estimate=cost(2 * len(held) * rows * depth * cols, 8 * depth * cols),
        )(order, *held, weight, base)

    near = add(stream, pieces[:3], 0, jnp.float32)
    return add(near, pieces[3:], 3, jnp.bfloat16)


def hidden_units_kernel(order_ref, p0, p1, p2, p3, gain_ref, gate_ref, up_ref, out_ref, norm_ref):
    @pl.when(pl.program_id(0) == 0)
    def _():
        wide = [ref[...].astype(jnp.float32) for ref in (p0, p1, p2, p3)]
        square = sum(jnp.sum(piece * piece, axis=1, keepdims=True) for piece in wide)
        scale = lax.rsqrt(square / (4 * p0.shape[1]) + epsilon)
        for place, piece in enumerate(wide):
            norm_ref[place] = (piece * scale * gain_ref[order_ref[place]]).astype(jnp.bfloat16)

    gated = jnp.zeros(out_ref.shape, jnp.float32)
    lifted = jnp.zeros(out_ref.shape, jnp.float32)
    for place in range(4):
        gated += jnp.dot(
            norm_ref[place], gate_ref[order_ref[place]], preferred_element_type=jnp.float32
        )
        lifted += jnp.dot(
            norm_ref[place], up_ref[order_ref[place]], preferred_element_type=jnp.float32
        )
    out_ref[...] = (gated / (1.0 + jnp.exp(-gated)) * lifted).astype(jnp.bfloat16)


def hidden_units(order, pieces, gain, gate, up):
    rows, width = pieces[0].shape
    depth, cols = gate.shape
    tile = cols // 2
    whole = vmem((rows, width), lambda j: (0, 0))
    strip = vmem((4, width, tile), lambda j: (0, 0, j))
    return kernel_call(
        hidden_units_kernel,
        out_shape=jax.ShapeDtypeStruct((rows, cols), jnp.bfloat16),
        grid=(2,),
        in_specs=[smem(), whole, whole, whole, whole, vmem((4, 1, width), lambda j: (0, 0, 0)), strip, strip],
        out_specs=vmem((rows, tile), lambda j: (0, j)),
        scratch_shapes=[pltpu.VMEM((4, rows, width), jnp.bfloat16)],
        compiler_params=params(24),
        cost_estimate=cost(4 * rows * depth * cols, 4 * depth * cols + 2 * rows * depth),
    )(
        order,
        *pieces,
        gain.reshape(4, 1, width),
        gate.reshape(4, width, cols),
        up.reshape(4, width, cols),
    )


def features_kernel(order_ref, p0, p1, p2, p3, down_ref, out_ref):
    total = jnp.zeros(out_ref.shape, jnp.float32)
    for place, ref in enumerate((p0, p1, p2, p3)):
        total += jnp.dot(ref[...], down_ref[order_ref[place]], preferred_element_type=jnp.float32)
    out_ref[...] = total.astype(out_ref.dtype)


def features(order, pieces, down, dtype):
    rows, width = pieces[0].shape
    depth, cols = down.shape
    return kernel_call(
        features_kernel,
        out_shape=jax.ShapeDtypeStruct((rows, cols), dtype),
        in_specs=[smem()] + [vmem()] * 5,
        out_specs=vmem(),
        compiler_params=params(24),
        cost_estimate=cost(2 * rows * depth * cols, 2 * depth * cols + 2 * rows * depth),
    )(order, *pieces, down.reshape(4, width, cols))


def pack_kernel(expert_ref, own_routes_ref, near_routes_ref, own_ref, near_ref, *outs):
    experts = len(outs)
    capacity = outs[0].shape[0] // 2
    rows = own_ref.shape[0]
    earlier = (
        lax.broadcasted_iota(jnp.int32, (rows, rows), 0)
        < lax.broadcasted_iota(jnp.int32, (rows, rows), 1)
    ).astype(jnp.bfloat16)
    slots = lax.broadcasted_iota(jnp.int32, (capacity, rows), 0)
    for half, (routes_ref, rows_ref) in enumerate(
        ((own_routes_ref, own_ref), (near_routes_ref, near_ref))
    ):
        routes = routes_ref[...]
        hits = jnp.concatenate(
            [
                jnp.max((routes == expert_ref[place]).astype(jnp.float32), axis=0, keepdims=True)
                for place in range(experts)
            ],
            axis=0,
        )
        ranks = jnp.dot(hits.astype(jnp.bfloat16), earlier, preferred_element_type=jnp.float32)
        ranks = jnp.where(hits > 0, ranks, -1.0).astype(jnp.int32)
        held = rows_ref[...]
        for place in range(experts):
            chosen = (slots == ranks[place : place + 1, :]).astype(jnp.bfloat16)
            outs[place][half * capacity : (half + 1) * capacity, :] = jnp.dot(
                chosen, held, preferred_element_type=jnp.float32
            ).astype(jnp.bfloat16)


def pack(experts, own_routes, near_routes, own, near, capacity):
    count = experts.shape[0]
    cols = own.shape[1]
    return kernel_call(
        pack_kernel,
        out_shape=[jax.ShapeDtypeStruct((2 * capacity, cols), jnp.bfloat16)] * count,
        in_specs=[smem()] + [vmem()] * 4,
        out_specs=[vmem()] * count,
        compiler_params=params(),
        cost_estimate=cost(4 * count * capacity * own.size, 8 * count * capacity * cols),
    )(experts, own_routes, near_routes, own, near)


def pack_near_kernel(expert_ref, own_routes_ref, near_routes_ref, *refs):
    pieces, outs = refs[:8], refs[8:]
    capacity = outs[0].shape[0] // 2
    rows = pieces[0].shape[0]
    earlier = (
        lax.broadcasted_iota(jnp.int32, (rows, rows), 0)
        < lax.broadcasted_iota(jnp.int32, (rows, rows), 1)
    ).astype(jnp.bfloat16)
    slots = lax.broadcasted_iota(jnp.int32, (capacity, rows), 0)
    for half, routes_ref in enumerate((own_routes_ref, near_routes_ref)):
        matches = (routes_ref[...] == expert_ref[0]).astype(jnp.float32)
        hit = jnp.max(matches, axis=0, keepdims=True)
        ranks = jnp.dot(
            jnp.broadcast_to(hit, (8, rows)).astype(jnp.bfloat16),
            earlier,
            preferred_element_type=jnp.float32,
        )[0:1]
        ranks = jnp.where(hit > 0, ranks, -1.0).astype(jnp.int32)
        chosen = (slots == ranks).astype(jnp.bfloat16)
        for place, out in enumerate(outs):
            out[half * capacity : (half + 1) * capacity, :] = jnp.dot(
                chosen, pieces[4 * half + place][...], preferred_element_type=jnp.float32
            ).astype(jnp.bfloat16)


def pack_near(experts, own_routes, near_routes, own, near, capacity):
    cols = own[0].shape[1]
    return kernel_call(
        pack_near_kernel,
        out_shape=[jax.ShapeDtypeStruct((2 * capacity, cols), jnp.bfloat16)] * 4,
        in_specs=[smem()] + [vmem()] * 10,
        out_specs=[vmem()] * 4,
        compiler_params=params(),
        cost_estimate=cost(16 * capacity * own[0].size, 16 * own[0].size),
    )(experts, own_routes, near_routes, *own, *near)


def spread_kernel(expert_ref, routes_ref, weights_ref, *refs, half):
    parts, out_ref = refs[:-1], refs[-1]
    rows = routes_ref.shape[0]
    capacity = parts[0].shape[0] // 2
    earlier = (
        lax.broadcasted_iota(jnp.int32, (rows, rows), 1)
        < lax.broadcasted_iota(jnp.int32, (rows, rows), 0)
    ).astype(jnp.bfloat16)
    slots = lax.broadcasted_iota(jnp.int32, (rows, capacity), 1)
    routes = routes_ref[...]
    weights = weights_ref[...]
    total = jnp.zeros(out_ref.shape, jnp.float32)
    for place, ref in enumerate(parts):
        matches = routes == expert_ref[place]
        hit = jnp.max(matches.astype(jnp.float32), axis=1, keepdims=True)
        share = jnp.sum(jnp.where(matches, weights, 0.0), axis=1, keepdims=True)
        rank = jnp.dot(
            earlier,
            jnp.broadcast_to(hit, (rows, capacity)).astype(jnp.bfloat16),
            preferred_element_type=jnp.float32,
        ).astype(jnp.int32)
        chosen = ((slots == rank) & (hit > 0)).astype(jnp.bfloat16)
        total += share * jnp.dot(
            chosen,
            ref[half * capacity : (half + 1) * capacity, :],
            preferred_element_type=jnp.float32,
        )
    out_ref[...] = total


def spread(experts, routes, weights, parts, half):
    rows = routes.shape[0]
    capacity, cols = parts[0].shape[0] // 2, parts[0].shape[1]
    return kernel_call(
        functools.partial(spread_kernel, half=half),
        out_shape=jax.ShapeDtypeStruct((rows, cols), jnp.float32),
        in_specs=[smem()] + [vmem()] * (2 + len(parts)),
        out_specs=vmem(),
        compiler_params=params(),
        cost_estimate=cost(4 * rows * capacity * cols * len(parts), 4 * capacity * cols * len(parts)),
    )(experts, routes, weights, *parts)


def finish_kernel(order_ref, p0, p1, p2, p3, down_ref, hidden_ref, own_ref, near_ref, out_ref):
    total = hidden_ref[...].astype(jnp.float32) + own_ref[...] + near_ref[...]
    for place, ref in enumerate((p0, p1, p2, p3)):
        total += jnp.dot(ref[...], down_ref[order_ref[place]], preferred_element_type=jnp.float32)
    out_ref[...] = total.astype(jnp.bfloat16)


def finish(order, pieces, down, hidden, own, near):
    rows, width = pieces[0].shape
    depth, cols = down.shape
    return kernel_call(
        finish_kernel,
        out_shape=jax.ShapeDtypeStruct((rows, cols), jnp.bfloat16),
        in_specs=[smem()] + [vmem()] * 8,
        out_specs=vmem(),
        compiler_params=params(24),
        cost_estimate=cost(2 * rows * depth * cols, 2 * depth * cols + 2 * rows * depth),
    )(order, *pieces, down.reshape(4, width, cols), hidden, own, near)


def swapped_shards(
    query_pairs,
    key_pairs,
    value_rows,
    doc_ids,
    contrast_lambda,
    head_gain,
    stream,
    out_proj,
    norm_gain,
    routes,
    route_weights,
    expert_gate,
    expert_up,
    expert_down,
    shared_gate,
    shared_up,
    shared_down,
):
    rows = query_pairs.shape[0]
    sp_size = lax.axis_size("sp")
    sp_at = lax.axis_index("sp")
    tp_at = lax.axis_index("tp")
    qk = query_pairs.shape[1] // sp_size
    value_width = value_rows.shape[1] // sp_size
    width = 2 * qk + value_width + 8
    order = jnp.bitwise_xor(tp_at, jnp.arange(4, dtype=jnp.int32))
    experts = jnp.bitwise_xor(sp_at, 2 * jnp.arange(sp_size // 2, dtype=jnp.int32))

    folded = kernel_call(
        fold_kernel,
        out_shape=jax.ShapeDtypeStruct((sp_size, width, rows), jnp.bfloat16),
        in_specs=[vmem()] * 4,
        out_specs=vmem(),
    )(query_pairs, key_pairs, value_rows, doc_ids.reshape(1, rows))
    blocks = lax.all_to_all(folded, "sp", split_axis=0, concat_axis=0, tiled=True)
    heard = kernel_call(
        functools.partial(attend_kernel, key_width=qk // 2),
        out_shape=jax.ShapeDtypeStruct((sp_size, value_width, rows), jnp.bfloat16),
        in_specs=[smem(), vmem(), vmem()],
        out_specs=vmem(),
        scratch_shapes=[
            pltpu.VMEM((sp_size * rows, qk), jnp.bfloat16),
            pltpu.VMEM((sp_size, rows, 128), jnp.float32),
            pltpu.VMEM((sp_size, 8, rows), jnp.float32),
            pltpu.SMEM((sp_size,), jnp.int32),
        ],
        compiler_params=params(),
        cost_estimate=cost(sp_size * sp_size * rows * rows * 128, 2 * blocks.size),
    )(lax.dynamic_slice_in_dim(contrast_lambda, sp_at, 1, 0), blocks, head_gain[:, None])
    back = lax.all_to_all(heard, "sp", split_axis=0, concat_axis=0, tiled=True)
    near_routes = swap(routes, "sp", 1)
    near_weights = swap(route_weights, "sp", 1)
    head_pieces = gather_pieces(back.reshape(sp_size * value_width, rows), 1)
    hidden = project(order, head_pieces, out_proj, stream)

    capacity = 2 * rows * routes.shape[1] // sp_size
    near_hidden = swap(hidden, "sp", 1)
    turned, near_turned = routes.T, near_routes.T
    packed = pack(experts[1:], turned, near_turned, hidden, near_hidden, capacity)
    shared_pieces = gather_pieces(hidden, 1)
    near_pieces = [near_hidden]
    for at in (1, 2, 3):
        near_pieces.append(swap(shared_pieces[at], "sp", 1))
    shared_units = hidden_units(order, shared_pieces, norm_gain, shared_gate, shared_up)
    parts = []
    for at in range(sp_size // 2):
        if at:
            relay = (1, 1, 2, 2)[at]
            held = swap(packed[at - 1], "sp", 2 * at)
            pieces = gather_pieces(held, relay)
        else:
            pieces = pack_near(experts, turned, near_turned, shared_pieces, near_pieces, capacity)
        units = hidden_units(order, pieces, norm_gain, expert_gate[0], expert_up[0])
        unit_pieces = gather_pieces(units, (2, 2, 1, 1)[at])
        outs = features(order, unit_pieces, expert_down[0], jnp.bfloat16)
        parts.append(swap(outs, "sp", 2 * at) if at else outs)
    for_near = spread(experts, near_routes, near_weights, parts, 1)
    for_own = spread(experts, routes, route_weights, parts, 0)
    shared_unit_pieces = gather_pieces(shared_units, 1)
    near_sum = swap(for_near, "sp", 1)
    return finish(order, shared_unit_pieces, shared_down, hidden, for_own, near_sum)


def solution(mesh):
    sp_size, tp_size = mesh.shape["sp"], mesh.shape["tp"]

    swapped = tp_size == 4 and sp_size == 8

    def body(*arrays):
        if swapped and arrays[4].shape[0] == sp_size:
            return swapped_shards(*arrays)
        return shards(*arrays)

    return jax.shard_map(
        body,
        mesh=mesh,
        in_specs=(
            P("sp", "tp"),
            P("sp", "tp"),
            P("sp", "tp"),
            P("sp"),
            P("tp"),
            P(),
            P("sp", "tp"),
            P(None, "tp"),
            P(),
            P("sp", None),
            P("sp", None),
            P("sp", None, "tp"),
            P("sp", None, "tp"),
            P("sp", None, "tp"),
            P(None, "tp"),
            P(None, "tp"),
            P(None, "tp"),
        ),
        out_specs=P("sp", "tp"),
        check_vma=False,
    )
```

```python
import functools
import math

import jax
import jax.numpy as jnp
from jax import lax
from jax.experimental import pallas as pl
from jax.experimental.pallas import tpu as pltpu

from jax.sharding import PartitionSpec as P

epsilon = 1e-06
floor_score = -1e30


def add_columns(weight_rows, part_block):
    return jnp.dot(part_block, weight_rows, preferred_element_type=jnp.float32)


def shards(
    query_pairs,
    key_pairs,
    value_rows,
    doc_ids,
    contrast_lambda,
    head_gain,
    stream,
    out_proj,
    norm_gain,
    routes,
    route_weights,
    expert_gate,
    expert_up,
    expert_down,
    shared_gate,
    shared_up,
    shared_down,
):
    row_count = query_pairs.shape[0]
    local_heads = contrast_lambda.shape[0]
    key_width = query_pairs.shape[1] // (2 * local_heads)
    value_width = value_rows.shape[1] // local_heads
    scaling = key_width ** (-0.5)
    first_row = lax.axis_index("sp") * row_count
    query_pos = first_row + jnp.arange(row_count, dtype=jnp.int32)
    last_query = first_row + row_count - 1
    first_doc = doc_ids[0]
    query_split = query_pairs.reshape(row_count, local_heads, 2, key_width)

    def absorb_block(running, key_block, value_block, doc_block, key_start):
        best, denom, numer = running
        span_len = key_block.shape[0]
        key_pos = key_start + jnp.arange(span_len, dtype=jnp.int32)
        allowed = (key_pos[None, :] <= query_pos[:, None]) & (
            doc_block[None, :] == doc_ids[:, None]
        )
        scores = (
            jnp.einsum(
                "qhmd,khmd->hmqk",
                query_split,
                key_block.reshape(span_len, local_heads, 2, key_width),
                preferred_element_type=jnp.float32,
            )
            * scaling
        )
        scores = jnp.where(allowed, scores, floor_score)
        new_best = jnp.maximum(best, jnp.max(scores, axis=-1))
        weights = jnp.where(allowed, jnp.exp(scores - new_best[..., None]), 0.0)
        fade = jnp.exp(best - new_best)
        denom = denom * fade + jnp.sum(weights, axis=-1)
        numer = numer * fade[..., None] + jnp.einsum(
            "hmqk,khv->hmqv",
            weights.astype(jnp.bfloat16),
            value_block.reshape(span_len, local_heads, value_width),
            preferred_element_type=jnp.float32,
        )
        return (new_best, denom, numer)

    start_best = jnp.full((local_heads, 2, row_count), floor_score, jnp.float32)
    start_denom = jnp.zeros((local_heads, 2, row_count), jnp.float32)
    start_numer = jnp.zeros((local_heads, 2, row_count, value_width), jnp.float32)
    key_piece = lax.all_gather(key_pairs, "sp", axis=0, tiled=True)
    value_piece = lax.all_gather(value_rows, "sp", axis=0, tiled=True)
    doc_piece = lax.all_gather(doc_ids, "sp", axis=0, tiled=True)
    length = key_piece.shape[0]
    span_len = row_count * max(1, 512 // row_count)

    def one_span(span_index, carried):
        offset = span_index * span_len
        key_block = lax.dynamic_slice_in_dim(key_piece, offset, span_len, 0)
        value_block = lax.dynamic_slice_in_dim(value_piece, offset, span_len, 0)
        doc_block = lax.dynamic_slice_in_dim(doc_piece, offset, span_len, 0)
        needed = (offset <= last_query) & (doc_block[span_len - 1] >= first_doc)
        return lax.cond(
            needed,
            lambda held: absorb_block(held, key_block, value_block, doc_block, offset),
            lambda held: held,
            carried,
        )

    _, denom, numer = lax.fori_loop(
        0, length // span_len, one_span, (start_best, start_denom, start_numer)
    )
    heard = numer / denom[..., None]
    contrast = heard[:, 0] - contrast_lambda[:, None, None] * heard[:, 1]
    contrast = (
        contrast
        * lax.rsqrt(jnp.mean(contrast * contrast, axis=-1, keepdims=True) + epsilon)
        * head_gain
    )
    head_out = (
        jnp.transpose(contrast, (1, 0, 2))
        .reshape(row_count, local_heads * value_width)
        .astype(jnp.bfloat16)
    )
    projected = add_columns(out_proj, lax.all_gather(head_out, "tp", axis=1, tiled=True))
    hidden_cols = (stream.astype(jnp.float32) + projected).astype(jnp.bfloat16)
    hidden_rows = lax.all_gather(hidden_cols, "tp", axis=1, tiled=True)
    widened = hidden_rows.astype(jnp.float32)
    normed = (
        widened
        * lax.rsqrt(jnp.mean(widened * widened, axis=-1, keepdims=True) + epsilon)
        * norm_gain
    ).astype(jnp.bfloat16)
    shared_act = (
        jax.nn.silu(jnp.dot(normed, shared_gate, preferred_element_type=jnp.float32))
        * jnp.dot(normed, shared_up, preferred_element_type=jnp.float32)
    ).astype(jnp.bfloat16)
    shared_cols = add_columns(shared_down, lax.all_gather(shared_act, "tp", axis=1, tiled=True))
    expert_count = lax.axis_size("sp")
    route_count = routes.shape[1]
    capacity = 2 * row_count * route_count // expert_count
    flat_routes = routes.reshape(-1)
    hits = (flat_routes[:, None] == jnp.arange(expert_count, dtype=jnp.int32)[None, :]).astype(
        jnp.int32
    )
    position = jnp.sum(jnp.cumsum(hits, axis=0) * hits, axis=1) - 1
    target = flat_routes * capacity + position
    sources = jnp.arange(flat_routes.shape[0], dtype=jnp.int32) // route_count
    owner = jnp.zeros((expert_count * capacity,), jnp.int32).at[target].set(sources)
    outgoing = normed[owner].reshape(expert_count, capacity, normed.shape[1])
    gate_cols = expert_gate[0]
    up_cols = expert_up[0]
    down_cols = expert_down[0]
    slice_width = outgoing.shape[2] // lax.axis_size("tp")
    own_slice = lax.dynamic_slice_in_dim(
        outgoing, lax.axis_index("tp") * slice_width, slice_width, 2
    )
    arrived = lax.all_to_all(own_slice, "sp", split_axis=0, concat_axis=0, tiled=True)
    apply_arrived = lax.all_gather(arrived, "tp", axis=2, tiled=True)
    gated = jnp.einsum("snd,df->snf", apply_arrived, gate_cols, preferred_element_type=jnp.float32)
    lifted = jnp.einsum("snd,df->snf", apply_arrived, up_cols, preferred_element_type=jnp.float32)
    expert_act = (jax.nn.silu(gated) * lifted).astype(jnp.bfloat16)
    expert_out = add_columns(
        down_cols, lax.all_gather(expert_act, "tp", axis=2, tiled=True)
    ).astype(jnp.bfloat16)
    returned = lax.all_to_all(expert_out, "sp", split_axis=0, concat_axis=0, tiled=True)
    flat_back = returned.reshape(expert_count * capacity, returned.shape[2])
    picked = (
        flat_back[target].reshape(row_count, route_count, returned.shape[2]).astype(jnp.float32)
    )
    routed = jnp.sum(picked * route_weights[:, :, None], axis=1)
    return (hidden_cols.astype(jnp.float32) + shared_cols + routed).astype(jnp.bfloat16)


def pair_swap(size, mask):
    return [(i, i ^ mask) for i in range(size)]


def swap(x, axis, mask):
    return lax.ppermute(x, axis, pair_swap(lax.axis_size(axis), mask))


def gather_pieces(own, relay):
    one = swap(own, "tp", 1)
    two = swap(own, "tp", 2)
    three = swap(one if relay == 2 else two, "tp", relay)
    return (own, one, two, three)


def kernel_call(body, **settings):
    def call(*operands):
        return pl.pallas_call(body, **settings)(*operands)

    return call


def vmem(shape=None, index_map=None):
    if shape is None:
        return pl.BlockSpec(memory_space=pltpu.VMEM)
    return pl.BlockSpec(shape, index_map)


def smem():
    return pl.BlockSpec(memory_space=pltpu.SMEM)


def cost(flops, nbytes):
    return pl.CostEstimate(flops=flops, bytes_accessed=nbytes, transcendentals=0)


def params(mebibytes=48):
    return pltpu.CompilerParams(vmem_limit_bytes=mebibytes * 1024 * 1024)


def fold_kernel(query_ref, key_ref, value_ref, doc_ref, out_ref):
    groups, width, rows = out_ref.shape
    for place, ref in enumerate((query_ref, key_ref, value_ref)):
        turned = ref[...].astype(jnp.float32).T.astype(jnp.bfloat16)
        each = turned.shape[0] // groups
        for group in range(groups):
            out_ref[group, place * each : (place + 1) * each, :] = turned[
                group * each : (group + 1) * each
            ]
    tail = 3 * (query_ref.shape[1] // groups)
    docs = jnp.broadcast_to(doc_ref[...].astype(jnp.bfloat16), (width - tail, rows))
    for group in range(groups):
        out_ref[group, tail:, :] = docs


def attend_kernel(
    lam_ref, block_ref, gain_ref, out_ref, keys_ref, cols_ref, rows_ref, low_ref, *, key_width
):
    blocks, _, rows = block_ref.shape
    qk = 2 * key_width
    value_width = out_ref.shape[1]
    power = key_width ** (-0.5) * math.log2(math.e)
    doc_rows = jnp.concatenate(
        [block_ref[b, qk * 2 + value_width :, :][0:1] for b in range(blocks)], axis=0
    ).astype(jnp.float32)
    doc_cols = doc_rows.T
    first_docs, last_docs = doc_rows[:, 0:1], doc_rows[:, rows - 1 : rows]
    for b in range(blocks):
        turned = block_ref[b, qk : 2 * qk, :].astype(jnp.float32).T
        keys_ref[b * rows : (b + 1) * rows, :] = turned.astype(jnp.bfloat16)
        cols_ref[b] = jnp.broadcast_to(doc_cols[:, b : b + 1], (rows, 128))
        rows_ref[b] = jnp.broadcast_to(doc_rows[b : b + 1], (8, rows))
        earlier = (last_docs < first_docs[b : b + 1]).astype(jnp.float32)
        low_ref[b] = jnp.sum(earlier).astype(jnp.int32)
    feature = lax.broadcasted_iota(jnp.int32, (qk, rows), 0)

    def one_block(q, _):
        turned = block_ref[q, 0:qk, :]
        zero = jnp.zeros_like(turned)
        halves = (
            jnp.where(feature < key_width, turned, zero),
            jnp.where(feature >= key_width, turned, zero),
        )
        query_docs = rows_ref[q][0:1]

        def absorb(k, carried, span):
            keys = keys_ref[pl.ds(pl.multiple_of(k * rows, rows), span * rows), :]
            docs = jnp.concatenate([cols_ref[k + b] for b in range(span)], axis=0)
            allowed = jnp.concatenate([docs] * (rows // 128), axis=1) == query_docs
            ahead = lax.broadcasted_iota(
                jnp.int32, (span * rows, rows), 0
            ) - lax.broadcasted_iota(jnp.int32, (span * rows, rows), 1)
            allowed &= ahead <= (q - k) * rows
            after = []
            raw = [jnp.dot(keys, half, preferred_element_type=jnp.float32) for half in halves]
            for scores, (best, denom, numer) in zip(raw, carried):
                scores = jnp.where(allowed, scores, floor_score)
                new_best = jnp.maximum(best, jnp.max(scores, axis=0, keepdims=True))
                weights = jnp.exp2((scores - new_best) * power)
                fade = jnp.exp2((best - new_best) * power)
                denom = denom * fade + jnp.sum(weights, axis=0, keepdims=True)
                rounded = weights.astype(jnp.bfloat16)
                numer = numer * fade
                for b in range(span):
                    numer += jnp.dot(
                        block_ref[k + b, 2 * qk : 2 * qk + value_width, :],
                        rounded[b * rows : (b + 1) * rows],
                        preferred_element_type=jnp.float32,
                    )
                after.append((new_best, denom, numer))
            return tuple(after)

        start = (
            jnp.full((1, rows), floor_score, jnp.float32),
            jnp.zeros((1, rows), jnp.float32),
            jnp.zeros((value_width, rows), jnp.float32),
        )
        low = low_ref[q]
        count = q + 1 - low
        carried = (start, start)
        for span, steps in (
            (1, lax.rem(count, 2)),
            (2, lax.div(lax.rem(count, 4), 2)),
            (4, lax.div(count, 4)),
        ):
            carried = lax.fori_loop(
                0,
                steps,
                lambda step, c, low=low, span=span: absorb(low + span * step, c, span),
                carried,
            )
            low += span * steps
        heard = [numer / denom for _, denom, numer in carried]
        contrast = heard[0] - lam_ref[0] * heard[1]
        mean = jnp.mean(contrast * contrast, axis=0, keepdims=True)
        out_ref[q] = (contrast * lax.rsqrt(mean + epsilon) * gain_ref[...]).astype(jnp.bfloat16)
        return 0

    lax.fori_loop(0, blocks, one_block, 0)


def project_kernel(order_ref, *refs, first):
    pieces, (weight_ref, base_ref, out_ref) = refs[:-3], refs[-3:]
    total = base_ref[...].astype(jnp.float32)
    for place, ref in enumerate(pieces):
        total += lax.dot_general(
            ref[...],
            weight_ref[order_ref[first + place]],
            (((0,), (0,)), ((), ())),
            preferred_element_type=jnp.float32,
        )
    out_ref[...] = total.astype(out_ref.dtype)


def project(order, pieces, weight, stream):
    rows, cols = stream.shape
    depth = weight.shape[0] // 4
    weight = weight.reshape(4, depth, cols)

    def add(base, held, first, dtype):
        return kernel_call(
            functools.partial(project_kernel, first=first),
            out_shape=jax.ShapeDtypeStruct((rows, cols), dtype),
            in_specs=[smem()] + [vmem()] * (2 + len(held)),
            out_specs=vmem(),
            compiler_params=params(32),
            cost_estimate=cost(2 * len(held) * rows * depth * cols, 8 * depth * cols),
        )(order, *held, weight, base)

    near = add(stream, pieces[:3], 0, jnp.float32)
    return add(near, pieces[3:], 3, jnp.bfloat16)


def hidden_units_kernel(order_ref, p0, p1, p2, p3, gain_ref, gate_ref, up_ref, out_ref, norm_ref):
    @pl.when(pl.program_id(0) == 0)
    def _():
        wide = [ref[...].astype(jnp.float32) for ref in (p0, p1, p2, p3)]
        square = sum(jnp.sum(piece * piece, axis=1, keepdims=True) for piece in wide)
        scale = lax.rsqrt(square / (4 * p0.shape[1]) + epsilon)
        for place, piece in enumerate(wide):
            norm_ref[place] = (piece * scale * gain_ref[order_ref[place]]).astype(jnp.bfloat16)

    gated = jnp.zeros(out_ref.shape, jnp.float32)
    lifted = jnp.zeros(out_ref.shape, jnp.float32)
    for place in range(4):
        gated += jnp.dot(
            norm_ref[place], gate_ref[order_ref[place]], preferred_element_type=jnp.float32
        )
        lifted += jnp.dot(
            norm_ref[place], up_ref[order_ref[place]], preferred_element_type=jnp.float32
        )
    out_ref[...] = (gated / (1.0 + jnp.exp(-gated)) * lifted).astype(jnp.bfloat16)


def hidden_units(order, pieces, gain, gate, up):
    rows, width = pieces[0].shape
    depth, cols = gate.shape
    tile = cols // 2
    whole = vmem((rows, width), lambda j: (0, 0))
    strip = vmem((4, width, tile), lambda j: (0, 0, j))
    return kernel_call(
        hidden_units_kernel,
        out_shape=jax.ShapeDtypeStruct((rows, cols), jnp.bfloat16),
        grid=(2,),
        in_specs=[smem(), whole, whole, whole, whole, vmem((4, 1, width), lambda j: (0, 0, 0)), strip, strip],
        out_specs=vmem((rows, tile), lambda j: (0, j)),
        scratch_shapes=[pltpu.VMEM((4, rows, width), jnp.bfloat16)],
        compiler_params=params(24),
        cost_estimate=cost(4 * rows * depth * cols, 4 * depth * cols + 2 * rows * depth),
    )(
        order,
        *pieces,
        gain.reshape(4, 1, width),
        gate.reshape(4, width, cols),
        up.reshape(4, width, cols),
    )


def features_kernel(order_ref, p0, p1, p2, p3, down_ref, out_ref):
    total = jnp.zeros(out_ref.shape, jnp.float32)
    for place, ref in enumerate((p0, p1, p2, p3)):
        total += jnp.dot(ref[...], down_ref[order_ref[place]], preferred_element_type=jnp.float32)
    out_ref[...] = total.astype(out_ref.dtype)


def features(order, pieces, down, dtype):
    rows, width = pieces[0].shape
    depth, cols = down.shape
    return kernel_call(
        features_kernel,
        out_shape=jax.ShapeDtypeStruct((rows, cols), dtype),
        in_specs=[smem()] + [vmem()] * 5,
        out_specs=vmem(),
        compiler_params=params(24),
        cost_estimate=cost(2 * rows * depth * cols, 2 * depth * cols + 2 * rows * depth),
    )(order, *pieces, down.reshape(4, width, cols))


def pack_kernel(expert_ref, own_routes_ref, near_routes_ref, own_ref, near_ref, *outs):
    experts = len(outs)
    capacity = outs[0].shape[0] // 2
    rows = own_ref.shape[0]
    earlier = (
        lax.broadcasted_iota(jnp.int32, (rows, rows), 0)
        < lax.broadcasted_iota(jnp.int32, (rows, rows), 1)
    ).astype(jnp.bfloat16)
    slots = lax.broadcasted_iota(jnp.int32, (capacity, rows), 0)
    for half, (routes_ref, rows_ref) in enumerate(
        ((own_routes_ref, own_ref), (near_routes_ref, near_ref))
    ):
        routes = routes_ref[...]
        hits = jnp.concatenate(
            [
                jnp.max((routes == expert_ref[place]).astype(jnp.float32), axis=0, keepdims=True)
                for place in range(experts)
            ],
            axis=0,
        )
        ranks = jnp.dot(hits.astype(jnp.bfloat16), earlier, preferred_element_type=jnp.float32)
        ranks = jnp.where(hits > 0, ranks, -1.0).astype(jnp.int32)
        held = rows_ref[...]
        for place in range(experts):
            chosen = (slots == ranks[place : place + 1, :]).astype(jnp.bfloat16)
            outs[place][half * capacity : (half + 1) * capacity, :] = jnp.dot(
                chosen, held, preferred_element_type=jnp.float32
            ).astype(jnp.bfloat16)


def pack(experts, own_routes, near_routes, own, near, capacity):
    count = experts.shape[0]
    cols = own.shape[1]
    return kernel_call(
        pack_kernel,
        out_shape=[jax.ShapeDtypeStruct((2 * capacity, cols), jnp.bfloat16)] * count,
        in_specs=[smem()] + [vmem()] * 4,
        out_specs=[vmem()] * count,
        compiler_params=params(),
        cost_estimate=cost(4 * count * capacity * own.size, 8 * count * capacity * cols),
    )(experts, own_routes, near_routes, own, near)


def pack_near_kernel(expert_ref, own_routes_ref, near_routes_ref, *refs):
    pieces, outs = refs[:8], refs[8:]
    capacity = outs[0].shape[0] // 2
    rows = pieces[0].shape[0]
    earlier = (
        lax.broadcasted_iota(jnp.int32, (rows, rows), 0)
        < lax.broadcasted_iota(jnp.int32, (rows, rows), 1)
    ).astype(jnp.bfloat16)
    slots = lax.broadcasted_iota(jnp.int32, (capacity, rows), 0)
    for half, routes_ref in enumerate((own_routes_ref, near_routes_ref)):
        matches = (routes_ref[...] == expert_ref[0]).astype(jnp.float32)
        hit = jnp.max(matches, axis=0, keepdims=True)
        ranks = jnp.dot(
            jnp.broadcast_to(hit, (8, rows)).astype(jnp.bfloat16),
            earlier,
            preferred_element_type=jnp.float32,
        )[0:1]
        ranks = jnp.where(hit > 0, ranks, -1.0).astype(jnp.int32)
        chosen = (slots == ranks).astype(jnp.bfloat16)
        for place, out in enumerate(outs):
            out[half * capacity : (half + 1) * capacity, :] = jnp.dot(
                chosen, pieces[4 * half + place][...], preferred_element_type=jnp.float32
            ).astype(jnp.bfloat16)


def pack_near(experts, own_routes, near_routes, own, near, capacity):
    cols = own[0].shape[1]
    return kernel_call(
        pack_near_kernel,
        out_shape=[jax.ShapeDtypeStruct((2 * capacity, cols), jnp.bfloat16)] * 4,
        in_specs=[smem()] + [vmem()] * 10,
        out_specs=[vmem()] * 4,
        compiler_params=params(),
        cost_estimate=cost(16 * capacity * own[0].size, 16 * own[0].size),
    )(experts, own_routes, near_routes, *own, *near)


def spread_kernel(expert_ref, routes_ref, weights_ref, *refs, half):
    parts, out_ref = refs[:-1], refs[-1]
    rows = routes_ref.shape[0]
    capacity = parts[0].shape[0] // 2
    earlier = (
        lax.broadcasted_iota(jnp.int32, (rows, rows), 1)
        < lax.broadcasted_iota(jnp.int32, (rows, rows), 0)
    ).astype(jnp.bfloat16)
    slots = lax.broadcasted_iota(jnp.int32, (rows, capacity), 1)
    routes = routes_ref[...]
    weights = weights_ref[...]
    total = jnp.zeros(out_ref.shape, jnp.float32)
    for place, ref in enumerate(parts):
        matches = routes == expert_ref[place]
        hit = jnp.max(matches.astype(jnp.float32), axis=1, keepdims=True)
        share = jnp.sum(jnp.where(matches, weights, 0.0), axis=1, keepdims=True)
        rank = jnp.dot(
            earlier,
            jnp.broadcast_to(hit, (rows, capacity)).astype(jnp.bfloat16),
            preferred_element_type=jnp.float32,
        ).astype(jnp.int32)
        chosen = ((slots == rank) & (hit > 0)).astype(jnp.bfloat16)
        total += share * jnp.dot(
            chosen,
            ref[half * capacity : (half + 1) * capacity, :],
            preferred_element_type=jnp.float32,
        )
    out_ref[...] = total


def spread(experts, routes, weights, parts, half):
    rows = routes.shape[0]
    capacity, cols = parts[0].shape[0] // 2, parts[0].shape[1]
    return kernel_call(
        functools.partial(spread_kernel, half=half),
        out_shape=jax.ShapeDtypeStruct((rows, cols), jnp.float32),
        in_specs=[smem()] + [vmem()] * (2 + len(parts)),
        out_specs=vmem(),
        compiler_params=params(),
        cost_estimate=cost(4 * rows * capacity * cols * len(parts), 4 * capacity * cols * len(parts)),
    )(experts, routes, weights, *parts)


def finish_kernel(order_ref, p0, p1, p2, p3, down_ref, hidden_ref, own_ref, near_ref, out_ref):
    total = hidden_ref[...].astype(jnp.float32) + own_ref[...] + near_ref[...]
    for place, ref in enumerate((p0, p1, p2, p3)):
        total += jnp.dot(ref[...], down_ref[order_ref[place]], preferred_element_type=jnp.float32)
    out_ref[...] = total.astype(jnp.bfloat16)


def finish(order, pieces, down, hidden, own, near):
    rows, width = pieces[0].shape
    depth, cols = down.shape
    return kernel_call(
        finish_kernel,
        out_shape=jax.ShapeDtypeStruct((rows, cols), jnp.bfloat16),
        in_specs=[smem()] + [vmem()] * 8,
        out_specs=vmem(),
        compiler_params=params(24),
        cost_estimate=cost(2 * rows * depth * cols, 2 * depth * cols + 2 * rows * depth),
    )(order, *pieces, down.reshape(4, width, cols), hidden, own, near)


def swapped_shards(
    query_pairs,
    key_pairs,
    value_rows,
    doc_ids,
    contrast_lambda,
    head_gain,
    stream,
    out_proj,
    norm_gain,
    routes,
    route_weights,
    expert_gate,
    expert_up,
    expert_down,
    shared_gate,
    shared_up,
    shared_down,
):
    rows = query_pairs.shape[0]
    sp_size = lax.axis_size("sp")
    sp_at = lax.axis_index("sp")
    tp_at = lax.axis_index("tp")
    qk = query_pairs.shape[1] // sp_size
    value_width = value_rows.shape[1] // sp_size
    width = 2 * qk + value_width + 8
    order = jnp.bitwise_xor(tp_at, jnp.arange(4, dtype=jnp.int32))
    experts = jnp.bitwise_xor(sp_at, 2 * jnp.arange(sp_size // 2, dtype=jnp.int32))

    folded = kernel_call(
        fold_kernel,
        out_shape=jax.ShapeDtypeStruct((sp_size, width, rows), jnp.bfloat16),
        in_specs=[vmem()] * 4,
        out_specs=vmem(),
    )(query_pairs, key_pairs, value_rows, doc_ids.reshape(1, rows))
    blocks = lax.all_to_all(folded, "sp", split_axis=0, concat_axis=0, tiled=True)
    heard = kernel_call(
        functools.partial(attend_kernel, key_width=qk // 2),
        out_shape=jax.ShapeDtypeStruct((sp_size, value_width, rows), jnp.bfloat16),
        in_specs=[smem(), vmem(), vmem()],
        out_specs=vmem(),
        scratch_shapes=[
            pltpu.VMEM((sp_size * rows, qk), jnp.bfloat16),
            pltpu.VMEM((sp_size, rows, 128), jnp.float32),
            pltpu.VMEM((sp_size, 8, rows), jnp.float32),
            pltpu.SMEM((sp_size,), jnp.int32),
        ],
        compiler_params=params(),
        cost_estimate=cost(sp_size * sp_size * rows * rows * 128, 2 * blocks.size),
    )(lax.dynamic_slice_in_dim(contrast_lambda, sp_at, 1, 0), blocks, head_gain[:, None])
    back = lax.all_to_all(heard, "sp", split_axis=0, concat_axis=0, tiled=True)
    near_routes = swap(routes, "sp", 1)
    near_weights = swap(route_weights, "sp", 1)
    head_pieces = gather_pieces(back.reshape(sp_size * value_width, rows), 1)
    hidden = project(order, head_pieces, out_proj, stream)

    capacity = 2 * rows * routes.shape[1] // sp_size
    near_hidden = swap(hidden, "sp", 1)
    turned, near_turned = routes.T, near_routes.T
    packed = pack(experts[1:], turned, near_turned, hidden, near_hidden, capacity)
    shared_pieces = gather_pieces(hidden, 1)
    near_pieces = [near_hidden]
    for at in (1, 2, 3):
        near_pieces.append(swap(shared_pieces[at], "sp", 1))
    shared_units = hidden_units(order, shared_pieces, norm_gain, shared_gate, shared_up)
    parts = []
    for at in range(sp_size // 2):
        if at:
            relay = (1, 1, 2, 2)[at]
            held = swap(packed[at - 1], "sp", 2 * at)
            pieces = gather_pieces(held, relay)
        else:
            pieces = pack_near(experts, turned, near_turned, shared_pieces, near_pieces, capacity)
        units = hidden_units(order, pieces, norm_gain, expert_gate[0], expert_up[0])
        unit_pieces = gather_pieces(units, (2, 2, 1, 1)[at])
        outs = features(order, unit_pieces, expert_down[0], jnp.bfloat16)
        parts.append(swap(outs, "sp", 2 * at) if at else outs)
    for_near = spread(experts, near_routes, near_weights, parts, 1)
    for_own = spread(experts, routes, route_weights, parts, 0)
    shared_unit_pieces = gather_pieces(shared_units, 1)
    near_sum = swap(for_near, "sp", 1)
    return finish(order, shared_unit_pieces, shared_down, hidden, for_own, near_sum)


def solution(mesh):
    sp_size, tp_size = mesh.shape["sp"], mesh.shape["tp"]

    swapped = tp_size == 4 and sp_size == 8

    def body(*arrays):
        if swapped and arrays[4].shape[0] == sp_size:
            return swapped_shards(*arrays)
        return shards(*arrays)

    return jax.shard_map(
        body,
        mesh=mesh,
        in_specs=(
            P("sp", "tp"),
            P("sp", "tp"),
            P("sp", "tp"),
            P("sp"),
            P("tp"),
            P(),
            P("sp", "tp"),
            P(None, "tp"),
            P(),
            P("sp", None),
            P("sp", None),
            P("sp", None, "tp"),
            P("sp", None, "tp"),
            P("sp", None, "tp"),
            P(None, "tp"),
            P(None, "tp"),
            P(None, "tp"),
        ),
        out_specs=P("sp", "tp"),
        check_vma=False,
    )
```
